32 devices in a mesh: tp: 8 (over z, y), dp: 4 (over x, core).
Axes of the slice: x: 2, y: 2, z: 4, core: 2. Of those that a mesh axis runs over, the one named last changes fastest.
Arguments:
- tokens: bfloat16 [96, 4096], P('tp', 'dp'), may hold values from -6 to 6
- lengths: int32 [24], P('dp'), may hold values from 1 to 4, 42 in all
- norm_gain: float32 [2, 4096], P(None, 'dp'), may hold values from 0.1 to 1.9
- gate_weight: bfloat16 [2, 4096, 8192], P(None, 'dp', 'tp'), may hold values from -0.09375 to 0.09375
- value_weight: bfloat16 [2, 4096, 8192], P(None, 'dp', 'tp'), may hold values from -0.09375 to 0.09375
- vector_weight: bfloat16 [2, 4096, 2, 2048], P(None, 'dp', None, 'tp'), may hold values from -0.09375 to 0.09375
- step_weight: bfloat16 [2, 4096, 128], P(None, 'dp'), may hold values from -0.09375 to 0.09375
- step_bias: float32 [2, 128], P(None, 'tp'), may hold values from -3 to 0
- decay_rate: float32 [2, 128], P(None, 'tp'), may hold values from 0.003 to 1
- value_taps: bfloat16 [2, 4, 8192], P(None, None, 'tp'), may hold values from -3 to 3
- vector_taps: bfloat16 [2, 4, 2, 2048], P(None, None, None, 'tp'), may hold values from -3 to 3
- out_weight: bfloat16 [2, 8192, 4096], P(None, 'tp', 'dp'), may hold values from -0.0625 to 0.0625
- recurrent_state: float32 [2, 24, 128, 64, 128], P(None, 'dp', 'tp'), may hold values from -4 to 4
- value_history: bfloat16 [2, 24, 3, 8192], P(None, 'dp', None, 'tp'), may hold values from -6 to 6
- vector_history: bfloat16 [2, 24, 3, 2, 2048], P(None, 'dp', None, None, 'tp'), may hold values from -6 to 6
Outputs:
- next_tokens: bfloat16 [96, 4096], P('tp', 'dp')
- next_state: float32 [2, 24, 128, 64, 128], P(None, 'dp', 'tp')
- next_value_history: bfloat16 [2, 24, 3, 8192], P(None, 'dp', None, 'tp')
- next_vector_history: bfloat16 [2, 24, 3, 2, 2048], P(None, 'dp', None, None, 'tp')
The draws below stay inside these ranges and needn't reach their ends.
Inputs may be any that keep to these rules, and one draw needn't show every extreme that they name: `lengths`: the number of live new tokens of each sequence; some sequences have more than twice the mean.
All inputs are finite; a program needn't handle non-finite values. No bound on the sum of `lengths` on one device may be relied on, other than what follows from the above.
Results may differ from the reference program's by a relative error of at most 0.029.
Values may be sent and summed in bfloat16 or wider, within the bound.
A program may use at most 128 MiB of HBM per device.

```python
import math
import jax
import jax.numpy as jnp
import numpy as np
from jax import lax

D = 4096
HEADS = 128
HEAD_DIM = 64
STATE = 128
GROUPS = 16
CONV = 4
NEW = 4
LAYERS = 2
SEQS = 24
TOKENS = 96


def steps_of(rng, shape, shards, least, top_value):
    loudness, own = 1.0, jax.random.fold_in(rng, 6)
    for position, shards_of in shards:
        draws = jnp.exp(jax.random.uniform(jax.random.fold_in(own, position), (shards_of,), jnp.float32, least / len(shards), top_value / len(shards)))
        loudness = loudness * jnp.repeat(draws, shape[position] // shards_of).reshape([-1 if axis == position else 1 for axis in range(len(shape))])
    return loudness


def length_profile(amount, total, reach, slope):
    weights = [(1 << 20) // math.isqrt(grade ** slope) + 1 for grade in range(2, amount + 1)]
    spare, counts = total - reach - (amount - 1), [1] * (amount - 1)
    while spare > 0:
        movable = [i for i in range(amount - 1) if counts[i] < reach]
        pool, budget = sum([weights[i] for i in movable]), spare
        for i in movable:
            addition = min(reach - counts[i], max(1, budget * weights[i] // pool), spare)
            counts[i] = counts[i] + addition
            spare = spare - addition
    return np.array([reach] + counts)


def ragged(own_key, number_of, total, reach, lean):
    if number_of == 2:
        one = jax.random.randint(own_key, (), max(1, total - reach), min(reach, total - 1) + 1)
        return jnp.stack([one, total - one])
    sizes = jnp.asarray(length_profile(number_of, total, reach, lean), jnp.int32)
    couples = (number_of - 1) // 2
    donor, receiver = sizes[1:1 + 2 * couples:2], sizes[2:2 + 2 * couples:2]
    slack = jnp.minimum(donor - 1, reach - receiver)
    passed = jax.random.randint(jax.random.fold_in(own_key, 1), (couples,), 0, 1 << 20) % (slack + 1)
    sizes = sizes.at[1:1 + 2 * couples:2].set(donor - passed).at[2:2 + 2 * couples:2].set(receiver + passed)
    return sizes[jax.random.permutation(jax.random.fold_in(own_key, 2), number_of)]


def scatter_about(key, extent, deviation, most, shards=(), kind=jnp.bfloat16):
    values = jax.random.normal(key, extent, jnp.float32) * deviation
    if len(shards) > 0:
        values = steps_of(key, extent, shards, -0.22, 0.18) * values
    return jnp.clip(values, min=-most, max=most).astype(kind)


def setup_inputs(seed: int = 0) -> dict:
    arg_keys = jax.random.split(jax.random.key(seed), 16)
    return {
        "tokens": scatter_about(arg_keys[0], (TOKENS, D), 1.0, 6.0, ((0, 8), (1, 4))),
        "lengths": ragged(arg_keys[1], SEQS, max(7 * SEQS // 4, SEQS + NEW - 1), NEW, 2).astype(jnp.int32),
        "norm_gain": jnp.clip(1.0 + 0.18 * jax.random.normal(arg_keys[2], (LAYERS, D), jnp.float32), 0.1, 1.9),
        "gate_weight": scatter_about(arg_keys[3], (LAYERS, D, HEADS * HEAD_DIM), D ** -0.5, 0.09375, ((1, 4), (2, 8))),
        "value_weight": scatter_about(arg_keys[4], (LAYERS, D, HEADS * HEAD_DIM), D ** -0.5, 0.09375, ((1, 4), (2, 8))),
        "vector_weight": scatter_about(arg_keys[5], (LAYERS, D, 2, GROUPS * STATE), D ** -0.5, 0.09375, ((1, 4), (3, 8))),
        "step_weight": scatter_about(arg_keys[6], (LAYERS, D, HEADS), D ** -0.5, 0.09375, ((1, 4),)),
        "step_bias": jnp.clip(-3.0 + 3.0 * jax.random.uniform(arg_keys[7], (LAYERS, HEADS), jnp.float32) ** steps_of(arg_keys[7], (LAYERS, HEADS), ((1, 8),), -0.2, 0.2), -3.0, 0.0),
        "decay_rate": jnp.clip(jnp.exp(math.log(1.0) - 5.809143 * jax.random.uniform(arg_keys[8], (LAYERS, HEADS), jnp.float32) ** steps_of(arg_keys[8], (LAYERS, HEADS), ((1, 8),), -0.2, 0.2)), 0.003, 1.0),
        "value_taps": scatter_about(arg_keys[9], (LAYERS, CONV, HEADS * HEAD_DIM), 0.5, 3.0, ((2, 8),)),
        "vector_taps": scatter_about(arg_keys[10], (LAYERS, CONV, 2, GROUPS * STATE), 0.5, 3.0, ((3, 8),)),
        "out_weight": scatter_about(arg_keys[11], (LAYERS, HEADS * HEAD_DIM, D), (HEADS * HEAD_DIM) ** -0.5, 0.0625, ((1, 8), (2, 4))),
        "recurrent_state": scatter_about(arg_keys[12], (LAYERS, SEQS, HEADS, HEAD_DIM, STATE), 0.5, 4.0, ((1, 4), (2, 8)), jnp.float32),
        "value_history": scatter_about(arg_keys[13], (LAYERS, SEQS, CONV - 1, HEADS * HEAD_DIM), 1.0, 6.0, ((1, 4), (3, 8))),
        "vector_history": scatter_about(arg_keys[14], (LAYERS, SEQS, CONV - 1, 2, GROUPS * STATE), 1.0, 6.0, ((1, 4), (4, 8))),
    }


norm_floor = 0.1
highest = lax.Precision.HIGHEST

def short_conv(history, fresh_rows, conv_taps):
    padded = jnp.concatenate([history, fresh_rows], axis=1)
    block_len = fresh_rows.shape[1]
    summed = jnp.zeros(fresh_rows.shape, jnp.float32)
    for offset in range(conv_taps.shape[0]):
        summed = summed + padded[:, offset:offset + block_len].astype(jnp.float32) * conv_taps[offset].astype(jnp.float32)
    return (jax.nn.silu(summed), padded)

def state_block(values, write_vec, read_vec, step_sizes, rate_vec, carried_state):
    block_len = values.shape[1]
    cumulative = jnp.cumsum(step_sizes * rate_vec, axis=1)
    causal = jnp.tril(jnp.ones((block_len, block_len), dtype=bool))[None, :, :, None, None]
    log_gap = cumulative[:, :, None] - cumulative[:, None, :]
    decays = jnp.where(causal, jnp.exp(-jnp.where(causal, log_gap, 0.0)), 0.0)
    scores = jnp.einsum('stgn,sugn->stug', read_vec, write_vec, precision=highest)
    weights = scores[..., None] * decays * step_sizes[:, None]
    within = jnp.einsum('stugr,sugrp->stgrp', weights, values, precision=highest)
    carried = jnp.einsum('stgn,sgrpn->stgrp', read_vec, carried_state, precision=highest) * jnp.exp(-cumulative)[..., None]
    ending = jnp.exp(cumulative - cumulative[:, -1:]) * step_sizes
    weighted = values * ending[..., None]
    fresh_state = jnp.einsum('sugrp,sugn->sgrpn', weighted, write_vec, precision=highest)
    next_state = carried_state * jnp.exp(-cumulative[:, -1])[..., None, None] + fresh_state
    return (within + carried, next_state)

def mixer_block(tokens, lengths, gain, gate_weight, value_weight, vector_weight, step_weight, step_bias, decay_rate, value_taps, vector_taps, out_weight, recurrent_state, value_history, vector_history):
    seq_count = lengths.shape[0]
    widened = tokens.astype(jnp.float32)
    scaling = lax.rsqrt(lax.optimization_barrier(jnp.mean(widened * widened, axis=1, keepdims=True)) + norm_floor)
    normed = (widened * gain).astype(jnp.bfloat16)

    def project(weight):
        return (jnp.dot(normed, weight, preferred_element_type=jnp.float32) * scaling).astype(jnp.bfloat16)
    gate = project(gate_weight)
    value_in = project(value_weight)
    vector_in = project(vector_weight.reshape(vector_weight.shape[0], -1))
    step_in = project(step_weight)
    live_mask = (jnp.arange(NEW, dtype=jnp.int32)[None, :] < lengths[:, None]).astype(jnp.float32)
    head_count = step_bias.shape[0]
    group_count = vector_weight.shape[2] // STATE
    per_group = head_count // group_count
    step_sizes = jax.nn.softplus(step_in.astype(jnp.float32).reshape(seq_count, NEW, head_count) + step_bias) * live_mask[:, :, None]
    value_conv, padded_value = short_conv(value_history, value_in.reshape(seq_count, NEW, -1), value_taps)
    vector_conv, padded_vector = short_conv(vector_history, vector_in.reshape(seq_count, NEW, 2, -1), vector_taps)
    write_vec = jnp.swapaxes(vector_conv[:, :, 0].reshape(seq_count, NEW, STATE, group_count), 2, 3)
    read_vec = jnp.swapaxes(vector_conv[:, :, 1].reshape(seq_count, NEW, STATE, group_count), 2, 3)
    output, next_state = state_block(value_conv.reshape(seq_count, NEW, group_count, per_group, HEAD_DIM), write_vec, read_vec, step_sizes.reshape(seq_count, NEW, group_count, per_group), decay_rate.reshape(group_count, per_group), recurrent_state.reshape(seq_count, group_count, per_group, HEAD_DIM, STATE))
    gated = output.reshape(seq_count, NEW, -1) * jax.nn.silu(gate.astype(jnp.float32).reshape(seq_count, NEW, -1)) * live_mask[:, :, None]
    mixed = gated.reshape(seq_count * NEW, -1).astype(jnp.bfloat16)
    update = jnp.dot(mixed, out_weight, preferred_element_type=jnp.float32)
    block_out = (widened + update).astype(jnp.bfloat16)
    kept_rows = lengths[:, None] + jnp.arange(CONV - 1, dtype=jnp.int32)[None, :]
    next_value = jnp.take_along_axis(padded_value, kept_rows[:, :, None], axis=1)
    next_vector = jnp.take_along_axis(padded_vector, kept_rows[:, :, None, None], axis=1)
    return (block_out, next_state.reshape(recurrent_state.shape), next_value, next_vector)

def reference(tokens, lengths, norm_gain, gate_weight, value_weight, vector_weight, step_weight, step_bias, decay_rate, value_taps, vector_taps, out_weight, recurrent_state, value_history, vector_history):
    current = tokens
    state_list, value_list, vector_list = ([], [], [])
    for ordinal in range(LAYERS):
        current, new_state, new_value, new_vector = mixer_block(current, lengths, norm_gain[ordinal], gate_weight[ordinal], value_weight[ordinal], vector_weight[ordinal], step_weight[ordinal], step_bias[ordinal], decay_rate[ordinal], value_taps[ordinal], vector_taps[ordinal], out_weight[ordinal], recurrent_state[ordinal], value_history[ordinal], vector_history[ordinal])
        state_list.append(new_state)
        value_list.append(new_value)
        vector_list.append(new_vector)
    return (current, jnp.stack(state_list), jnp.stack(value_list), jnp.stack(vector_list))
```

```python
import functools

import jax
import jax.numpy as jnp
from jax import lax
from jax.experimental import pallas as pl
from jax.experimental.pallas import tpu as pltpu
from jax.sharding import PartitionSpec as P

D = 4096
HEADS = 128
HEAD_DIM = 64
STATE = 128
GROUPS = 16
CONV = 4
NEW = 4
LAYERS = 2


norm_floor = 0.1
highest = lax.Precision.HIGHEST


def short_conv(history, fresh_rows, conv_taps):
    padded = jnp.concatenate([history, fresh_rows], axis=1)
    block_len = fresh_rows.shape[1]
    summed = jnp.zeros(fresh_rows.shape, jnp.float32)
    for offset in range(conv_taps.shape[0]):
        summed = summed + padded[:, offset : offset + block_len].astype(jnp.float32) * conv_taps[
            offset
        ].astype(jnp.float32)
    return (jax.nn.silu(summed), padded)


def state_block(values, write_vec, read_vec, step_sizes, rate_vec, carried_state):
    block_len = values.shape[1]
    cumulative = jnp.cumsum(step_sizes * rate_vec, axis=1)
    causal = jnp.tril(jnp.ones((block_len, block_len), dtype=bool))[None, :, :, None, None]
    log_gap = cumulative[:, :, None] - cumulative[:, None, :]
    decays = jnp.where(causal, jnp.exp(-jnp.where(causal, log_gap, 0.0)), 0.0)
    scores = jnp.einsum("stgn,sugn->stug", read_vec, write_vec, precision=highest)
    weights = scores[..., None] * decays * step_sizes[:, None]
    within = jnp.einsum("stugr,sugrp->stgrp", weights, values, precision=highest)
    carried = (
        jnp.einsum("stgn,sgrpn->stgrp", read_vec, carried_state, precision=highest)
        * jnp.exp(-cumulative)[..., None]
    )
    ending = jnp.exp(cumulative - cumulative[:, -1:]) * step_sizes
    weighted = values * ending[..., None]
    fresh_state = jnp.einsum("sugrp,sugn->sgrpn", weighted, write_vec, precision=highest)
    next_state = carried_state * jnp.exp(-cumulative[:, -1])[..., None, None] + fresh_state
    return (within + carried, next_state)


def collect(token_rows):
    return lax.all_gather(token_rows, "tp", axis=0, tiled=True)


def body(
    tokens,
    lengths,
    norm_gain,
    gate_weight,
    value_weight,
    vector_weight,
    step_weight,
    step_bias,
    decay_rate,
    value_taps,
    vector_taps,
    out_weight,
    recurrent_state,
    value_history,
    vector_history,
):
    local_seqs = lengths.shape[0]
    local_heads = step_bias.shape[1]
    local_tokens = local_seqs * NEW
    heads_group = HEADS // GROUPS
    group_count = max(1, local_heads // heads_group)
    per_group = local_heads // group_count
    live_mask = (jnp.arange(NEW, dtype=jnp.int32)[None, :] < lengths[:, None]).astype(jnp.float32)
    kept_rows = lengths[:, None] + jnp.arange(CONV - 1, dtype=jnp.int32)[None, :]
    picker = (
        kept_rows[:, :, None] == jnp.arange(CONV - 1 + NEW, dtype=jnp.int32)[None, None, :]
    ).astype(jnp.bfloat16)
    head_start = lax.axis_index("tp") * local_heads
    first_group = head_start // heads_group
    token_rows = tokens
    whole = collect(tokens)
    state_list, value_list, vector_list = ([], [], [])
    for ordinal in range(LAYERS):
        widened = whole.astype(jnp.float32)
        squares = jnp.sum(widened * widened, axis=1)
        normed = (widened * norm_gain[ordinal]).astype(jnp.bfloat16)
        own_step = lax.dynamic_slice_in_dim(step_weight[ordinal], head_start, local_heads, 1)
        gate_part = jnp.dot(normed, gate_weight[ordinal], preferred_element_type=jnp.float32)
        value_part = jnp.dot(normed, value_weight[ordinal], preferred_element_type=jnp.float32)
        vector_part = jnp.einsum(
            "td,dkc->tkc", normed, vector_weight[ordinal], preferred_element_type=jnp.float32
        )
        step_part = jnp.dot(normed, own_step, preferred_element_type=jnp.float32)
        gate_sum, value_sum, vector_sum, step_sum, own_squares = (
            lax.psum_scatter(gate_part, "dp", scatter_dimension=0, tiled=True),
            lax.psum_scatter(value_part, "dp", scatter_dimension=0, tiled=True),
            lax.psum_scatter(vector_part, "dp", scatter_dimension=0, tiled=True),
            lax.psum_scatter(step_part, "dp", scatter_dimension=0, tiled=True),
            lax.psum_scatter(squares, "dp", scatter_dimension=0, tiled=True),
        )
        scaling = lax.rsqrt(own_squares / D + norm_floor)[:, None]
        gate = (gate_sum * scaling).astype(jnp.bfloat16)
        value_in = (value_sum * scaling).astype(jnp.bfloat16)
        vector_in = (vector_sum * scaling[:, :, None]).astype(jnp.bfloat16)
        step_in = (step_sum * scaling).astype(jnp.bfloat16)
        step_sizes = (
            jax.nn.softplus(
                step_in.astype(jnp.float32).reshape(local_seqs, NEW, local_heads)
                + step_bias[ordinal]
            )
            * live_mask[:, :, None]
        )
        value_conv, padded_value = short_conv(
            value_history[ordinal], value_in.reshape(local_seqs, NEW, -1), value_taps[ordinal]
        )
        vector_conv, padded_vector = short_conv(
            vector_history[ordinal], vector_in.reshape(local_seqs, NEW, 2, -1), vector_taps[ordinal]
        )
        vector_whole = lax.all_gather(vector_conv, "tp", axis=3, tiled=True)
        arranged = vector_whole.reshape(local_seqs, NEW, 2, STATE, GROUPS)
        own_vectors = lax.dynamic_slice_in_dim(arranged, first_group, group_count, 4)
        write_vec = jnp.swapaxes(own_vectors[:, :, 0], 2, 3)
        read_vec = jnp.swapaxes(own_vectors[:, :, 1], 2, 3)
        output, next_state = state_block(
            value_conv.reshape(local_seqs, NEW, group_count, per_group, HEAD_DIM),
            write_vec,
            read_vec,
            step_sizes.reshape(local_seqs, NEW, group_count, per_group),
            decay_rate[ordinal].reshape(group_count, per_group),
            recurrent_state[ordinal].reshape(local_seqs, group_count, per_group, HEAD_DIM, STATE),
        )
        state_list.append(next_state.reshape(recurrent_state.shape[1:]))
        value_list.append(
            jnp.einsum(
                "sjk,skc->sjc", picker, padded_value, preferred_element_type=jnp.float32
            ).astype(jnp.bfloat16)
        )
        vector_list.append(
            jnp.einsum(
                "sjk,skmc->sjmc", picker, padded_vector, preferred_element_type=jnp.float32
            ).astype(jnp.bfloat16)
        )
        gated = (
            output.reshape(local_seqs, NEW, -1)
            * jax.nn.silu(gate.astype(jnp.float32).reshape(local_seqs, NEW, -1))
            * live_mask[:, :, None]
        )
        mixed = gated.reshape(local_tokens, -1).astype(jnp.bfloat16)
        mixed_all = lax.all_gather(mixed, "dp", axis=0, tiled=True)
        layer_out = out_weight[ordinal]
        update = lax.psum_scatter(
            jnp.dot(mixed_all, layer_out, preferred_element_type=jnp.float32),
            "tp",
            scatter_dimension=0,
            tiled=True,
        )
        token_rows = (token_rows.astype(jnp.float32) + update).astype(jnp.bfloat16)
        if ordinal + 1 < LAYERS:
            whole = collect(token_rows)
    return (token_rows, jnp.stack(state_list), jnp.stack(value_list), jnp.stack(vector_list))


BF = jnp.bfloat16
F32 = jnp.float32
SUB = 8


def one_hot(cond):
    return jnp.where(cond, 1.0, 0.0).astype(BF)


def grid_of(shape, dim):
    return lax.broadcasted_iota(jnp.int32, shape, dim)


def dot(a, b):
    return jnp.dot(a, b, preferred_element_type=F32)


def dot_nt(a, b):
    return lax.dot_general(a, b, (((1,), (1,)), ((), ())), preferred_element_type=F32)


def silu(x):
    return x * (1.0 / (1.0 + jnp.exp(-x)))


def softplus(x):
    return jnp.maximum(x, 0.0) + jnp.log1p(jnp.exp(-jnp.abs(x)))


def conv_rows(old, fresh, taps):
    padded = [old[SUB * k : SUB * (k + 1)] for k in range(CONV - 1)]
    padded = padded + [fresh[SUB * t : SUB * (t + 1)] for t in range(NEW)]
    outs = []
    for t in range(NEW):
        total = padded[t] * taps[0:1]
        for k in range(1, CONV):
            total = total + padded[t + k] * taps[k : k + 1]
        outs.append(silu(total))
    return outs, padded


def keep_rows(padded, lens):
    rows = []
    for j in range(CONV - 1):
        row = padded[j]
        for length in range(1, NEW + 1):
            row = jnp.where(lens == length, padded[length + j], row)
        rows.append(row)
    return jnp.concatenate(rows, axis=0)


def step_kernel(
    n_tp, n_dp, sizes,
    tok_ref, lens_ref, gain_ref, bias_ref, rate_ref, vtap_ref, ctap_ref, vhist_ref, chist_ref,
    gw_hbm, vw_hbm, cw_hbm, sw_hbm, ow_hbm, st_hbm,
    out_ref, nvh_ref, nch_ref, zt_ref, wr_ref,
    gw, vw, cw, sw, ow, st, whole, x32, tok, send_c, recv_c, send_v, recv_v, send_g, recv_g,
    send_w, recv_w, send_m, recv_m, acc, send_o, recv_o,
    load_sem, own_sem, ag_s, ag_r, rs_s, rs_r, vx_s, vx_r, mx_s, mx_r, ox_s, ox_r,
):
    rows, seqs = sizes
    block = seqs * NEW
    chans = vw.shape[2]
    vcols = cw.shape[2] // 2
    me_tp, me_dp = lax.axis_index("tp"), lax.axis_index("dp")
    barrier = pltpu.get_barrier_semaphore()
    for k in range(1, n_tp):
        pl.semaphore_signal(
            barrier, inc=1, device_id={"tp": lax.rem(me_tp + k, n_tp)},
            device_id_type=pl.DeviceIdType.MESH,
        )
    for k in range(1, n_dp):
        pl.semaphore_signal(
            barrier, inc=1, device_id={"dp": lax.rem(me_dp + k, n_dp)},
            device_id_type=pl.DeviceIdType.MESH,
        )
    loads = {}
    for layer in range(LAYERS):
        for slot, (name, src, dst) in enumerate(
            (("c", cw_hbm, cw), ("s", sw_hbm, sw), ("v", vw_hbm, vw), ("g", gw_hbm, gw),
             ("st", st_hbm, st), ("o", ow_hbm, ow))
        ):
            copy = pltpu.make_async_copy(src.at[layer], dst.at[layer], load_sem.at[layer, slot])
            copy.start()
            loads[layer, name] = copy
    pl.semaphore_wait(barrier, n_tp + n_dp - 2)
    pending = []

    def exchange(axis, n, me, source, target, s_sem, r_sem):
        waits = []
        for k in range(1, n):
            peer = lax.rem(me + k, n)
            copy = pltpu.make_async_remote_copy(
                src_ref=source(peer), dst_ref=target.at[me], send_sem=s_sem.at[k],
                recv_sem=r_sem.at[k], device_id={axis: peer},
                device_id_type=pl.DeviceIdType.MESH,
            )
            copy.start()
            pending.append(copy)
            origin = lax.rem(me + n - k, n)
            waits.append(
                pltpu.make_async_remote_copy(
                    src_ref=target.at[origin], dst_ref=target.at[origin], send_sem=s_sem.at[k],
                    recv_sem=r_sem.at[k], device_id={axis: peer},
                    device_id_type=pl.DeviceIdType.MESH,
                )
            )
        return waits

    lens = lens_ref[:, 0:1]
    live = [jnp.where(lens > t, 1.0, 0.0) for t in range(NEW)]
    big = NEW * SUB
    pr, pc = grid_of((big, block), 0), grid_of((big, block), 1)
    spread = one_hot(((pr & (SUB - 1)) < seqs) & (pc == (pr & (SUB - 1)) * NEW + (pr >> 3)))
    qr, qc = grid_of((block, big), 0), grid_of((block, big), 1)
    gather = one_hot((qr >> 2) + (qr & (NEW - 1)) * SUB == qc)
    heads_all = sw.shape[2]
    er, ec = grid_of((heads_all, chans), 0), grid_of((heads_all, chans), 1)
    expand = one_hot(er == me_tp * (chans // HEAD_DIM) + ec // HEAD_DIM)
    orow, ocol = grid_of((vcols, vcols), 0), grid_of((vcols, vcols), 1)
    part_n = vcols // GROUPS
    perm = one_hot(ocol == (orow & (part_n - 1)) * GROUPS + orow // part_n)
    groups = GROUPS // n_tp
    per = chans // groups
    seq_of_row = grid_of((big, STATE), 0) & (SUB - 1)

    for layer in range(LAYERS):
        mine = tok_ref if layer == 0 else tok
        wide = whole.at[layer]
        waits = exchange("tp", n_tp, me_tp, lambda peer: mine, wide, ag_s.at[layer], ag_r.at[layer])
        own = pltpu.make_async_copy(mine, wide.at[me_tp], own_sem.at[layer])
        own.start()
        own.wait()
        for w in waits:
            w.wait_recv()
        for i in range(n_tp):
            x32[rows * i : rows * (i + 1), :] = wide[i].astype(F32)
        x = x32[...]
        squares = jnp.sum(x * x, axis=1, keepdims=True)
        normed = (x * gain_ref[layer : layer + 1]).astype(BF)

        def scatter(parts, send, recv, which):
            at = 0
            for part in parts:
                width = part.shape[1]
                for d in range(n_dp):
                    send[layer, d, :, at : at + width] = part[block * d : block * (d + 1)].astype(BF)
                at = at + width
            return exchange(
                "dp", n_dp, me_dp, lambda peer: send.at[layer, peer], recv.at[layer],
                rs_s.at[layer, which], rs_r.at[layer, which],
            )

        def settle(waits, send, recv):
            total = send[layer, me_dp].astype(F32)
            for k, w in enumerate(waits):
                w.wait_recv()
                total = total + recv[layer, lax.rem(me_dp + n_dp - 1 - k, n_dp)].astype(F32)
            return total

        loads[layer, "c"].wait()
        vec_part = dot(normed, cw[layer])
        loads[layer, "s"].wait()
        step_part = dot(normed, sw[layer])
        lane = grid_of((rows * n_tp, 128), 1)
        high = squares.astype(BF).astype(F32)
        sq_part = jnp.where(lane == 0, high, jnp.where(lane == 1, squares - high, 0.0))
        waits_c = scatter((vec_part, step_part, sq_part), send_c, recv_c, 0)
        loads[layer, "v"].wait()
        waits_v = scatter((dot(normed, vw[layer]),), send_v, recv_v, 1)
        loads[layer, "g"].wait()
        waits_g = scatter((dot(normed, gw[layer]),), send_g, recv_g, 2)

        sums = settle(waits_c, send_c, recv_c)
        vwide = 2 * vcols
        total_sq = jnp.sum(sums[:, vwide + heads_all :], axis=1, keepdims=True)
        scaling = lax.rsqrt(total_sq / D + norm_floor)
        small = dot(spread, (sums[:, : vwide + heads_all] * scaling).astype(BF))
        conv, padded = conv_rows(
            chist_ref[layer].astype(F32), small[:, :vwide], ctap_ref[layer]
        )
        nch_ref[layer] = keep_rows(padded, lens).astype(BF)
        conv = jnp.concatenate(conv, axis=0)
        stacked = jnp.concatenate(
            [conv[:, :vcols], conv[:, vcols:], jnp.zeros((128 - 2 * big, vcols), F32)], axis=0
        ).astype(BF)
        turned = dot_nt(perm, stacked).astype(BF)
        each = vcols // n_tp
        for j in range(n_tp):
            send_w[layer, j] = turned[each * j : each * (j + 1)]
        waits_w = exchange(
            "tp", n_tp, me_tp, lambda peer: send_w.at[layer, peer], recv_w.at[layer],
            vx_s.at[layer], vx_r.at[layer],
        )
        recv_w[layer, me_tp] = send_w[layer, me_tp]

        steps_wide = dot(expand_rows(small, vwide), expand) + bias_ref[layer : layer + 1]
        steps_wide = softplus(steps_wide)
        step = [steps_wide[SUB * t : SUB * (t + 1)] * live[t] for t in range(NEW)]
        rate = rate_ref[layer : layer + 1]
        cum = [step[0] * rate]
        for t in range(1, NEW):
            cum.append(cum[-1] + step[t] * rate)
        values_in = dot(spread, (settle(waits_v, send_v, recv_v) * scaling).astype(BF))
        value, padded = conv_rows(vhist_ref[layer].astype(F32), values_in, vtap_ref[layer])
        nvh_ref[layer] = keep_rows(padded, lens).astype(BF)
        stepped = [step[t] * value[t] for t in range(NEW)]
        ending = [jnp.exp(cum[t] - cum[NEW - 1]) * stepped[t] for t in range(NEW)]
        gate_in = dot(spread, (settle(waits_g, send_g, recv_g) * scaling).astype(BF))
        gates = silu(gate_in)
        zrows = jnp.concatenate(
            ending + [jnp.exp(-cum[NEW - 1]), jnp.zeros((128 - big - SUB, chans), F32)], axis=0
        )
        zt_ref[layer] = zrows.T

        for w in waits_w:
            w.wait_recv()
        loads[layer, "st"].wait()
        half = each // groups
        y_parts = [[] for _ in range(NEW)]
        for g in range(groups):
            tall = jnp.concatenate(
                [recv_w[layer, i, half * g : half * (g + 1), :].astype(F32) for i in range(n_tp)],
                axis=0,
            )
            flat = tall.T
            write, read = flat[:big], flat[big : 2 * big]
            wr_ref[layer, g] = write.astype(BF)
            carried = jnp.zeros((big, per), F32)
            for s in range(seqs):
                picked = jnp.where(seq_of_row == s, read, 0.0).astype(BF)
                carried = carried + dot_nt(
                    picked, st[layer, s, per * g : per * (g + 1), :].astype(BF)
                )
            span = slice(per * g, per * (g + 1))
            for t in range(NEW):
                now = cum[t][:, span]
                y = carried[SUB * t : SUB * (t + 1)] * jnp.exp(-now)
                for u in range(t + 1):
                    score = jnp.sum(
                        read[SUB * t : SUB * (t + 1)] * write[SUB * u : SUB * (u + 1)],
                        axis=1, keepdims=True,
                    )
                    y = y + score * jnp.exp(cum[u][:, span] - now) * stepped[u][:, span]
                y_parts[t].append(y)
        mixed = jnp.concatenate(
            [
                jnp.concatenate(y_parts[t], axis=1) * gates[SUB * t : SUB * (t + 1)] * live[t]
                for t in range(NEW)
            ],
            axis=0,
        ).astype(BF)
        send_m[layer] = dot(gather, mixed).astype(BF)
        waits = exchange(
            "dp", n_dp, me_dp, lambda peer: send_m.at[layer], recv_m.at[layer],
            mx_s.at[layer], mx_r.at[layer],
        )
        recv_m[layer, me_dp] = send_m[layer]
        for w in waits:
            w.wait_recv()
        loads[layer, "o"].wait()
        mixed_all = jnp.concatenate([recv_m[layer, d] for d in range(n_dp)], axis=0)
        acc[...] = dot(mixed_all, ow[layer])
        for j in range(n_tp):
            send_o[layer, j] = acc[rows * j : rows * (j + 1), :].astype(BF)
        waits = exchange(
            "tp", n_tp, me_tp, lambda peer: send_o.at[layer, peer], recv_o.at[layer],
            ox_s.at[layer], ox_r.at[layer],
        )
        total = send_o[layer, me_tp].astype(F32)
        for k, w in enumerate(waits):
            w.wait_recv()
            total = total + recv_o[layer, lax.rem(me_tp + n_tp - 1 - k, n_tp)].astype(F32)
        fresh = (mine[...].astype(F32) + total).astype(BF)
        if layer + 1 < LAYERS:
            tok[...] = fresh
        else:
            out_ref[...] = fresh
    for copy in pending:
        copy.wait_send()


def expand_rows(small, start):
    return small[:, start:].astype(BF)


def state_kernel(seqs, zt_ref, wr_ref, st_ref, out_ref):
    zt = zt_ref[0]
    big = NEW * SUB
    weighted = zt[:, :big].astype(BF)
    write = wr_ref[0, 0].astype(F32)
    seq_of_row = grid_of((big, STATE), 0) & (SUB - 1)
    for s in range(seqs):
        picked = jnp.where(seq_of_row == s, write, 0.0).astype(BF)
        out_ref[0, s] = zt[:, big + s : big + s + 1] * st_ref[0, s] + dot(weighted, picked)


def fast_body(
    n_tp, n_dp,
    tokens, lengths, norm_gain, gate_weight, value_weight, vector_weight, step_weight, step_bias,
    decay_rate, value_taps, vector_taps, out_weight, recurrent_state, value_history, vector_history,
):
    rows, feats = tokens.shape
    seqs = lengths.shape[0]
    block = seqs * NEW
    chans = value_weight.shape[2]
    vwide = 2 * vector_weight.shape[3]
    heads_all = step_weight.shape[2]
    lens = jnp.broadcast_to(jnp.pad(lengths, (0, SUB - seqs))[:, None], (SUB, 128))
    wide_bias = jnp.repeat(step_bias, HEAD_DIM, axis=1)
    wide_rate = jnp.repeat(decay_rate, HEAD_DIM, axis=1)
    pad = ((0, 0), (0, 0), (0, SUB - seqs), (0, 0))
    vhist = jnp.pad(jnp.swapaxes(value_history, 1, 2), pad).reshape(LAYERS, -1, chans)
    chist = vector_history.reshape(LAYERS, seqs, CONV - 1, vwide)
    chist = jnp.pad(jnp.swapaxes(chist, 1, 2), pad).reshape(LAYERS, -1, vwide)
    state = recurrent_state.reshape(LAYERS, seqs, chans, STATE)
    groups = GROUPS // n_tp
    big = NEW * SUB
    csum = vwide + heads_all + 128
    vm, hb = pl.BlockSpec(memory_space=pltpu.VMEM), pl.BlockSpec(memory_space=pl.ANY)
    dma = pltpu.SemaphoreType.DMA
    each = vwide // 2 // n_tp
    fresh, nvh, nch, zt, wr = pl.pallas_call(
        functools.partial(step_kernel, n_tp, n_dp, (rows, seqs)),
        out_shape=(
            jax.ShapeDtypeStruct((rows, feats), BF),
            jax.ShapeDtypeStruct((LAYERS, (CONV - 1) * SUB, chans), BF),
            jax.ShapeDtypeStruct((LAYERS, (CONV - 1) * SUB, vwide), BF),
            jax.ShapeDtypeStruct((LAYERS, chans, 128), F32),
            jax.ShapeDtypeStruct((LAYERS, groups, big, STATE), BF),
        ),
        in_specs=[vm] * 9 + [hb] * 6,
        out_specs=(vm,) * 5,
        scratch_shapes=[
            pltpu.VMEM((LAYERS, feats, chans), BF),
            pltpu.VMEM((LAYERS, feats, chans), BF),
            pltpu.VMEM((LAYERS, feats, vwide), BF),
            pltpu.VMEM((LAYERS, feats, heads_all), BF),
            pltpu.VMEM((LAYERS, chans, feats), BF),
            pltpu.VMEM((LAYERS, seqs, chans, STATE), F32),
            pltpu.VMEM((LAYERS, n_tp, rows, feats), BF),
            pltpu.VMEM((n_tp * rows, feats), F32),
            pltpu.VMEM((rows, feats), BF),
            pltpu.VMEM((LAYERS, n_dp, block, csum), BF),
            pltpu.VMEM((LAYERS, n_dp, block, csum), BF),
            pltpu.VMEM((LAYERS, n_dp, block, chans), BF),
            pltpu.VMEM((LAYERS, n_dp, block, chans), BF),
            pltpu.VMEM((LAYERS, n_dp, block, chans), BF),
            pltpu.VMEM((LAYERS, n_dp, block, chans), BF),
            pltpu.VMEM((LAYERS, n_tp, each, 128), BF),
            pltpu.VMEM((LAYERS, n_tp, each, 128), BF),
            pltpu.VMEM((LAYERS, block, chans), BF),
            pltpu.VMEM((LAYERS, n_dp, block, chans), BF),
            pltpu.VMEM((n_tp * rows, feats), F32),
            pltpu.VMEM((LAYERS, n_tp, rows, feats), BF),
            pltpu.VMEM((LAYERS, n_tp, rows, feats), BF),
            dma((LAYERS, 6)),
            dma((LAYERS,)),
            dma((LAYERS, n_tp)), dma((LAYERS, n_tp)),
            dma((LAYERS, 3, n_dp)), dma((LAYERS, 3, n_dp)),
            dma((LAYERS, n_tp)), dma((LAYERS, n_tp)),
            dma((LAYERS, n_dp)), dma((LAYERS, n_dp)),
            dma((LAYERS, n_tp)), dma((LAYERS, n_tp)),
        ],
        compiler_params=pltpu.CompilerParams(
            collective_id=0, has_side_effects=True, vmem_limit_bytes=56 * 1024 * 1024
        ),
        name="step_kernel",
    )(
        tokens, lens, norm_gain, wide_bias, wide_rate, value_taps.astype(F32),
        vector_taps.reshape(LAYERS, CONV, vwide).astype(F32), vhist, chist,
        gate_weight, value_weight, vector_weight.reshape(LAYERS, feats, vwide), step_weight,
        out_weight, state,
    )
    cut = chans // groups // 2
    next_state = pl.pallas_call(
        functools.partial(state_kernel, seqs),
        grid=(LAYERS, chans // cut),
        out_shape=jax.ShapeDtypeStruct(state.shape, F32),
        in_specs=[
            pl.BlockSpec((1, cut, 128), lambda l, c: (l, c, 0)),
            pl.BlockSpec((1, 1, big, STATE), lambda l, c: (l, c // 2, 0, 0)),
            pl.BlockSpec((1, seqs, cut, STATE), lambda l, c: (l, 0, c, 0)),
        ],
        out_specs=pl.BlockSpec((1, seqs, cut, STATE), lambda l, c: (l, 0, c, 0)),
        name="state_kernel",
    )(zt, wr, state)

    def unpack(rows_of, width):
        return jnp.swapaxes(rows_of.reshape(LAYERS, CONV - 1, SUB, width)[:, :, :seqs], 1, 2)

    return (
        fresh,
        next_state.reshape(recurrent_state.shape),
        unpack(nvh, chans),
        unpack(nch, vwide).reshape(vector_history.shape),
    )


def choose(n_tp, n_dp, *args):
    tokens, lengths = args[0], args[1]
    fits = (
        GROUPS % n_tp == 0
        and args[7].shape[1] * n_tp == HEADS
        and args[5].shape[3] % 128 == 0
        and tokens.shape[1] % 128 == 0
        and tokens.shape[0] % 4 == 0
        and lengths.shape[0] <= SUB
        and args[5].shape[3] // GROUPS >= 16
        and tokens.shape[0] * n_tp == lengths.shape[0] * NEW * n_dp
    )
    if fits:
        return fast_body(n_tp, n_dp, *args)
    return body(*args)


def solution(mesh):
    return jax.shard_map(
        functools.partial(choose, mesh.shape['tp'], mesh.shape['dp']),
        mesh=mesh,
        in_specs=(
            P("tp", "dp"),
            P("dp"),
            P(None, "dp"),
            P(None, "dp", "tp"),
            P(None, "dp", "tp"),
            P(None, "dp", None, "tp"),
            P(None, "dp", None),
            P(None, "tp"),
            P(None, "tp"),
            P(None, None, "tp"),
            P(None, None, None, "tp"),
            P(None, "tp", "dp"),
            P(None, "dp", "tp", None, None),
            P(None, "dp", None, "tp"),
            P(None, "dp", None, None, "tp"),
        ),
        out_specs=(
            P("tp", "dp"),
            P(None, "dp", "tp", None, None),
            P(None, "dp", None, "tp"),
            P(None, "dp", None, None, "tp"),
        ),
        check_vma=False,
    )
```

```python
import functools

import jax
import jax.numpy as jnp
from jax import lax
from jax.experimental import pallas as pl
from jax.experimental.pallas import tpu as pltpu
from jax.sharding import PartitionSpec as P

D = 4096
HEADS = 128
HEAD_DIM = 64
STATE = 128
GROUPS = 16
CONV = 4
NEW = 4
LAYERS = 2


norm_floor = 0.1
highest = lax.Precision.HIGHEST


def short_conv(history, fresh_rows, conv_taps):
    padded = jnp.concatenate([history, fresh_rows], axis=1)
    block_len = fresh_rows.shape[1]
    summed = jnp.zeros(fresh_rows.shape, jnp.float32)
    for offset in range(conv_taps.shape[0]):
        summed = summed + padded[:, offset : offset + block_len].astype(jnp.float32) * conv_taps[
            offset
        ].astype(jnp.float32)
    return (jax.nn.silu(summed), padded)


def state_block(values, write_vec, read_vec, step_sizes, rate_vec, carried_state):
    block_len = values.shape[1]
    cumulative = jnp.cumsum(step_sizes * rate_vec, axis=1)
    causal = jnp.tril(jnp.ones((block_len, block_len), dtype=bool))[None, :, :, None, None]
    log_gap = cumulative[:, :, None] - cumulative[:, None, :]
    decays = jnp.where(causal, jnp.exp(-jnp.where(causal, log_gap, 0.0)), 0.0)
    scores = jnp.einsum("stgn,sugn->stug", read_vec, write_vec, precision=highest)
    weights = scores[..., None] * decays * step_sizes[:, None]
    within = jnp.einsum("stugr,sugrp->stgrp", weights, values, precision=highest)
    carried = (
        jnp.einsum("stgn,sgrpn->stgrp", read_vec, carried_state, precision=highest)
        * jnp.exp(-cumulative)[..., None]
    )
    ending = jnp.exp(cumulative - cumulative[:, -1:]) * step_sizes
    weighted = values * ending[..., None]
    fresh_state = jnp.einsum("sugrp,sugn->sgrpn", weighted, write_vec, precision=highest)
    next_state = carried_state * jnp.exp(-cumulative[:, -1])[..., None, None] + fresh_state
    return (within + carried, next_state)


def collect(token_rows):
    return lax.all_gather(token_rows, "tp", axis=0, tiled=True)


def body(
    tokens,
    lengths,
    norm_gain,
    gate_weight,
    value_weight,
    vector_weight,
    step_weight,
    step_bias,
    decay_rate,
    value_taps,
    vector_taps,
    out_weight,
    recurrent_state,
    value_history,
    vector_history,
):
    local_seqs = lengths.shape[0]
    local_heads = step_bias.shape[1]
    local_tokens = local_seqs * NEW
    heads_group = HEADS // GROUPS
    group_count = max(1, local_heads // heads_group)
    per_group = local_heads // group_count
    live_mask = (jnp.arange(NEW, dtype=jnp.int32)[None, :] < lengths[:, None]).astype(jnp.float32)
    kept_rows = lengths[:, None] + jnp.arange(CONV - 1, dtype=jnp.int32)[None, :]
    picker = (
        kept_rows[:, :, None] == jnp.arange(CONV - 1 + NEW, dtype=jnp.int32)[None, None, :]
    ).astype(jnp.bfloat16)
    head_start = lax.axis_index("tp") * local_heads
    first_group = head_start // heads_group
    token_rows = tokens
    whole = collect(tokens)
    state_list, value_list, vector_list = ([], [], [])
    for ordinal in range(LAYERS):
        widened = whole.astype(jnp.float32)
        squares = jnp.sum(widened * widened, axis=1)
        normed = (widened * norm_gain[ordinal]).astype(jnp.bfloat16)
        own_step = lax.dynamic_slice_in_dim(step_weight[ordinal], head_start, local_heads, 1)
        gate_part = jnp.dot(normed, gate_weight[ordinal], preferred_element_type=jnp.float32)
        value_part = jnp.dot(normed, value_weight[ordinal], preferred_element_type=jnp.float32)
        vector_part = jnp.einsum(
            "td,dkc->tkc", normed, vector_weight[ordinal], preferred_element_type=jnp.float32
        )
        step_part = jnp.dot(normed, own_step, preferred_element_type=jnp.float32)
        gate_sum, value_sum, vector_sum, step_sum, own_squares = (
            lax.psum_scatter(gate_part, "dp", scatter_dimension=0, tiled=True),
            lax.psum_scatter(value_part, "dp", scatter_dimension=0, tiled=True),
            lax.psum_scatter(vector_part, "dp", scatter_dimension=0, tiled=True),
            lax.psum_scatter(step_part, "dp", scatter_dimension=0, tiled=True),
            lax.psum_scatter(squares, "dp", scatter_dimension=0, tiled=True),
        )
        scaling = lax.rsqrt(own_squares / D + norm_floor)[:, None]
        gate = (gate_sum * scaling).astype(jnp.bfloat16)
        value_in = (value_sum * scaling).astype(jnp.bfloat16)
        vector_in = (vector_sum * scaling[:, :, None]).astype(jnp.bfloat16)
        step_in = (step_sum * scaling).astype(jnp.bfloat16)
        step_sizes = (
            jax.nn.softplus(
                step_in.astype(jnp.float32).reshape(local_seqs, NEW, local_heads)
                + step_bias[ordinal]
            )
            * live_mask[:, :, None]
        )
        value_conv, padded_value = short_conv(
            value_history[ordinal], value_in.reshape(local_seqs, NEW, -1), value_taps[ordinal]
        )
        vector_conv, padded_vector = short_conv(
            vector_history[ordinal], vector_in.reshape(local_seqs, NEW, 2, -1), vector_taps[ordinal]
        )
        vector_whole = lax.all_gather(vector_conv, "tp", axis=3, tiled=True)
        arranged = vector_whole.reshape(local_seqs, NEW, 2, STATE, GROUPS)
        own_vectors = lax.dynamic_slice_in_dim(arranged, first_group, group_count, 4)
        write_vec = jnp.swapaxes(own_vectors[:, :, 0], 2, 3)
        read_vec = jnp.swapaxes(own_vectors[:, :, 1], 2, 3)
        output, next_state = state_block(
            value_conv.reshape(local_seqs, NEW, group_count, per_group, HEAD_DIM),
            write_vec,
            read_vec,
            step_sizes.reshape(local_seqs, NEW, group_count, per_group),
            decay_rate[ordinal].reshape(group_count, per_group),
            recurrent_state[ordinal].reshape(local_seqs, group_count, per_group, HEAD_DIM, STATE),
        )
        state_list.append(next_state.reshape(recurrent_state.shape[1:]))
        value_list.append(
            jnp.einsum(
                "sjk,skc->sjc", picker, padded_value, preferred_element_type=jnp.float32
            ).astype(jnp.bfloat16)
        )
        vector_list.append(
            jnp.einsum(
                "sjk,skmc->sjmc", picker, padded_vector, preferred_element_type=jnp.float32
            ).astype(jnp.bfloat16)
        )
        gated = (
            output.reshape(local_seqs, NEW, -1)
            * jax.nn.silu(gate.astype(jnp.float32).reshape(local_seqs, NEW, -1))
            * live_mask[:, :, None]
        )
        mixed = gated.reshape(local_tokens, -1).astype(jnp.bfloat16)
        mixed_all = lax.all_gather(mixed, "dp", axis=0, tiled=True)
        layer_out = out_weight[ordinal]
        update = lax.psum_scatter(
            jnp.dot(mixed_all, layer_out, preferred_element_type=jnp.float32),
            "tp",
            scatter_dimension=0,
            tiled=True,
        )
        token_rows = (token_rows.astype(jnp.float32) + update).astype(jnp.bfloat16)
        if ordinal + 1 < LAYERS:
            whole = collect(token_rows)
    return (token_rows, jnp.stack(state_list), jnp.stack(value_list), jnp.stack(vector_list))


BF = jnp.bfloat16
F32 = jnp.float32
SUB = 8


def one_hot(cond):
    return jnp.where(cond, 1.0, 0.0).astype(BF)


def grid_of(shape, dim):
    return lax.broadcasted_iota(jnp.int32, shape, dim)


def dot(a, b):
    return jnp.dot(a, b, preferred_element_type=F32)


def dot_nt(a, b):
    return lax.dot_general(a, b, (((1,), (1,)), ((), ())), preferred_element_type=F32)


def silu(x):
    return x * (1.0 / (1.0 + jnp.exp(-x)))


def softplus(x):
    return jnp.maximum(x, 0.0) + jnp.log1p(jnp.exp(-jnp.abs(x)))


def conv_rows(old, fresh, taps):
    padded = [old[SUB * k : SUB * (k + 1)] for k in range(CONV - 1)]
    padded = padded + [fresh[SUB * t : SUB * (t + 1)] for t in range(NEW)]
    outs = []
    for t in range(NEW):
        total = padded[t] * taps[0]
        for k in range(1, CONV):
            total = total + padded[t + k] * taps[k]
        outs.append(silu(total))
    return outs, padded


def keep_rows(padded, lens):
    rows = []
    for j in range(CONV - 1):
        row = padded[j]
        for length in range(1, NEW + 1):
            row = jnp.where(lens == length, padded[length + j], row)
        rows.append(row)
    return jnp.concatenate(rows, axis=0)


def step_kernel(
    n_tp, n_dp, sizes,
    tok_ref, lens_ref, gain_ref, bias_ref, rate_ref, vtap_ref, ctap_ref, vhist_ref, chist_ref,
    gw_hbm, vw_hbm, cw_hbm, sw_hbm, ow_hbm, st_hbm,
    out_ref, nvh_ref, nch_ref, zt_ref, wr_ref,
    gw, vw, cw, raw, vhs, chs, sw, ow, st, whole, x32, tok, send_c, recv_c, send_v, recv_v, send_g, recv_g,
    send_w, recv_w, send_m, recv_m, acc, send_o, recv_o,
    load_sem, own_sem, ag_s, ag_r, rs_s, rs_r, vx_s, vx_r, mx_s, mx_r, ox_s, ox_r,
):
    rows, seqs = sizes
    block = seqs * NEW
    chans = vw.shape[2]
    vcols = cw.shape[2] // 2
    me_tp, me_dp = lax.axis_index("tp"), lax.axis_index("dp")
    barrier = pltpu.get_barrier_semaphore()
    for k in range(1, n_tp):
        pl.semaphore_signal(
            barrier, inc=1, device_id={"tp": lax.rem(me_tp + k, n_tp)},
            device_id_type=pl.DeviceIdType.MESH,
        )
    for k in range(1, n_dp):
        pl.semaphore_signal(
            barrier, inc=1, device_id={"dp": lax.rem(me_dp + k, n_dp)},
            device_id_type=pl.DeviceIdType.MESH,
        )
    loads = {}
    for layer in range(LAYERS):
        for slot, (name, src, dst) in enumerate(
            (("c", cw_hbm, raw), ("s", sw_hbm, sw), ("v", vw_hbm, vw), ("g", gw_hbm, gw),
             ("st", st_hbm, st), ("o", ow_hbm, ow))
        ):
            copy = pltpu.make_async_copy(src.at[layer], dst.at[layer], load_sem.at[layer, slot])
            copy.start()
            loads[layer, name] = copy
    pl.semaphore_wait(barrier, n_tp + n_dp - 2)
    pending = []

    def exchange(axis, n, me, source, target, s_sem, r_sem):
        waits = []
        for k in range(1, n):
            peer = lax.rem(me + k, n)
            copy = pltpu.make_async_remote_copy(
                src_ref=source(peer), dst_ref=target.at[me], send_sem=s_sem.at[k],
                recv_sem=r_sem.at[k], device_id={axis: peer},
                device_id_type=pl.DeviceIdType.MESH,
            )
            copy.start()
            pending.append(copy)
            origin = lax.rem(me + n - k, n)
            waits.append(
                pltpu.make_async_remote_copy(
                    src_ref=target.at[origin], dst_ref=target.at[origin], send_sem=s_sem.at[k],
                    recv_sem=r_sem.at[k], device_id={axis: peer},
                    device_id_type=pl.DeviceIdType.MESH,
                )
            )
        return waits

    who = grid_of((SUB, 128), 0)
    lens = jnp.zeros((SUB, 128), jnp.int32)
    for s in range(seqs):
        lens = jnp.where(who == s, lens_ref[s], lens)
    lens = lens[:, 0:1]
    live = [jnp.where(lens > t, 1.0, 0.0) for t in range(NEW)]
    big = NEW * SUB
    pr, pc = grid_of((big, block), 0), grid_of((big, block), 1)
    spread = one_hot(((pr & (SUB - 1)) < seqs) & (pc == (pr & (SUB - 1)) * NEW + (pr >> 3)))
    qr, qc = grid_of((block, big), 0), grid_of((block, big), 1)
    gather = one_hot((qr >> 2) + (qr & (NEW - 1)) * SUB == qc)
    heads_all = sw.shape[2]
    er, ec = grid_of((heads_all, chans), 0), grid_of((heads_all, chans), 1)
    expand = one_hot(er == me_tp * (chans // HEAD_DIM) + ec // HEAD_DIM)
    orow, ocol = grid_of((vcols, vcols), 0), grid_of((vcols, vcols), 1)
    part_n = vcols // GROUPS
    perm = one_hot(ocol == (orow & (part_n - 1)) * GROUPS + orow // part_n)
    local = chans // HEAD_DIM
    widen = one_hot(grid_of((local, chans), 0) == grid_of((local, chans), 1) // HEAD_DIM)
    left = jnp.concatenate([bias_ref[...], rate_ref[...]], axis=0)
    per_head = jnp.zeros((2 * LAYERS, chans), F32)
    for _ in range(3):
        piece = left.astype(BF)
        per_head = per_head + dot(piece, widen)
        left = left - piece.astype(F32)
    groups = GROUPS // n_tp
    per = chans // groups
    seq_of_row = grid_of((big, STATE), 0) & (SUB - 1)

    for layer in range(LAYERS):
        mine = tok_ref if layer == 0 else tok
        wide = whole.at[layer]
        waits = exchange("tp", n_tp, me_tp, lambda peer: mine, wide, ag_s.at[layer], ag_r.at[layer])
        own = pltpu.make_async_copy(mine, wide.at[me_tp], own_sem.at[layer])
        own.start()
        own.wait()
        if layer == 0:
            vhs[...] = jnp.zeros_like(vhs)
            chs[...] = jnp.zeros_like(chs)
            for s in range(seqs):
                for j in range(CONV - 1):
                    row = SUB * j + s
                    pair = vhist_ref[s, j].astype(F32)
                    for l in range(LAYERS):
                        vhs[l, row : row + 1, :] = pair[l : l + 1]
                        both = chist_ref[l, s, j].astype(F32)
                        chs[l, row : row + 1, :] = jnp.concatenate([both[0:1], both[1:2]], axis=1)
            for l in range(LAYERS):
                loads[l, "c"].wait()
                cut = 64

                def untangle(i, carry):
                    at = pl.multiple_of(i * cut, cut)
                    some = raw[l, pl.ds(at, cut)].astype(F32)
                    cw[l, pl.ds(at, cut), :] = jnp.concatenate(
                        [some[:, 0, :], some[:, 1, :]], axis=1
                    ).astype(BF)
                    return carry

                lax.fori_loop(0, raw.shape[1] // cut, untangle, 0)
        for w in waits:
            w.wait_recv()
        for i in range(n_tp):
            x32[rows * i : rows * (i + 1), :] = wide[i].astype(F32)
        x = x32[...]
        squares = jnp.sum(x * x, axis=1, keepdims=True)
        normed = (x * gain_ref[layer : layer + 1]).astype(BF)

        def scatter(parts, send, recv, which):
            at = 0
            for part in parts:
                width = part.shape[1]
                for d in range(n_dp):
                    send[layer, d, :, at : at + width] = part[block * d : block * (d + 1)].astype(BF)
                at = at + width
            return exchange(
                "dp", n_dp, me_dp, lambda peer: send.at[layer, peer], recv.at[layer],
                rs_s.at[layer, which], rs_r.at[layer, which],
            )

        def settle(waits, send, recv):
            total = send[layer, me_dp].astype(F32)
            for k, w in enumerate(waits):
                w.wait_recv()
                total = total + recv[layer, lax.rem(me_dp + n_dp - 1 - k, n_dp)].astype(F32)
            return total

        vec_part = dot(normed, cw[layer])
        loads[layer, "s"].wait()
        step_part = dot(normed, sw[layer])
        lane = grid_of((rows * n_tp, 128), 1)
        high = squares.astype(BF).astype(F32)
        sq_part = jnp.where(lane == 0, high, jnp.where(lane == 1, squares - high, 0.0))
        waits_c = scatter((vec_part, step_part, sq_part), send_c, recv_c, 0)
        loads[layer, "v"].wait()
        waits_v = scatter((dot(normed, vw[layer]),), send_v, recv_v, 1)
        loads[layer, "g"].wait()
        waits_g = scatter((dot(normed, gw[layer]),), send_g, recv_g, 2)

        sums = settle(waits_c, send_c, recv_c)
        vwide = 2 * vcols
        total_sq = jnp.sum(sums[:, vwide + heads_all :], axis=1, keepdims=True)
        scaling = lax.rsqrt(total_sq / D + norm_floor)
        small = dot(spread, (sums[:, : vwide + heads_all] * scaling).astype(BF))
        conv, padded = conv_rows(
            chs[layer], small[:, :vwide],
            [
                jnp.concatenate([ctap_ref[layer, k, 0:1], ctap_ref[layer, k, 1:2]], axis=1).astype(F32)
                for k in range(CONV)
            ],
        )
        nch_ref[layer] = keep_rows(padded, lens)
        conv = jnp.concatenate(conv, axis=0)
        stacked = jnp.concatenate(
            [conv[:, :vcols], conv[:, vcols:], jnp.zeros((128 - 2 * big, vcols), F32)], axis=0
        ).astype(BF)
        turned = dot_nt(perm, stacked).astype(BF)
        each = vcols // n_tp
        for j in range(n_tp):
            send_w[layer, j] = turned[each * j : each * (j + 1)]
        waits_w = exchange(
            "tp", n_tp, me_tp, lambda peer: send_w.at[layer, peer], recv_w.at[layer],
            vx_s.at[layer], vx_r.at[layer],
        )
        recv_w[layer, me_tp] = send_w[layer, me_tp]

        steps_wide = dot(expand_rows(small, vwide), expand) + per_head[layer : layer + 1]
        steps_wide = softplus(steps_wide)
        step = [steps_wide[SUB * t : SUB * (t + 1)] * live[t] for t in range(NEW)]
        rate = per_head[LAYERS + layer : LAYERS + layer + 1]
        cum = [step[0] * rate]
        for t in range(1, NEW):
            cum.append(cum[-1] + step[t] * rate)
        values_in = dot(spread, (settle(waits_v, send_v, recv_v) * scaling).astype(BF))
        value, padded = conv_rows(
            vhs[layer], values_in, [vtap_ref[layer, k : k + 1].astype(F32) for k in range(CONV)]
        )
        nvh_ref[layer] = keep_rows(padded, lens)
        stepped = [step[t] * value[t] for t in range(NEW)]
        ending = [jnp.exp(cum[t] - cum[NEW - 1]) * stepped[t] for t in range(NEW)]
        gate_in = dot(spread, (settle(waits_g, send_g, recv_g) * scaling).astype(BF))
        gates = silu(gate_in)
        fade = jnp.exp(-cum[NEW - 1])
        fade_high = fade.astype(BF).astype(F32)
        zrows = jnp.concatenate(
            ending + [fade_high, fade - fade_high, jnp.zeros((128 - big - 2 * SUB, chans), F32)],
            axis=0,
        )
        zt_ref[layer] = zrows.T.astype(BF)

        for w in waits_w:
            w.wait_recv()
        loads[layer, "st"].wait()
        half = each // groups
        y_parts = [[] for _ in range(NEW)]
        for g in range(groups):
            tall = jnp.concatenate(
                [recv_w[layer, i, half * g : half * (g + 1), :].astype(F32) for i in range(n_tp)],
                axis=0,
            )
            flat = tall.T
            write, read = flat[:big], flat[big : 2 * big]
            wr_ref[layer, g] = write.astype(BF)
            carried = jnp.zeros((big, per), F32)
            for s in range(seqs):
                picked = jnp.where(seq_of_row == s, read, 0.0).astype(BF)
                carried = carried + dot_nt(
                    picked, st[layer, s, per * g : per * (g + 1), :].astype(BF)
                )
            span = slice(per * g, per * (g + 1))
            for t in range(NEW):
                now = cum[t][:, span]
                y = carried[SUB * t : SUB * (t + 1)] * jnp.exp(-now)
                for u in range(t + 1):
                    score = jnp.sum(
                        read[SUB * t : SUB * (t + 1)] * write[SUB * u : SUB * (u + 1)],
                        axis=1, keepdims=True,
                    )
                    y = y + score * jnp.exp(cum[u][:, span] - now) * stepped[u][:, span]
                y_parts[t].append(y)
        mixed = jnp.concatenate(
            [
                jnp.concatenate(y_parts[t], axis=1) * gates[SUB * t : SUB * (t + 1)] * live[t]
                for t in range(NEW)
            ],
            axis=0,
        ).astype(BF)
        send_m[layer] = dot(gather, mixed).astype(BF)
        waits = exchange(
            "dp", n_dp, me_dp, lambda peer: send_m.at[layer], recv_m.at[layer],
            mx_s.at[layer], mx_r.at[layer],
        )
        recv_m[layer, me_dp] = send_m[layer]
        for w in waits:
            w.wait_recv()
        loads[layer, "o"].wait()
        mixed_all = jnp.concatenate([recv_m[layer, d] for d in range(n_dp)], axis=0)
        acc[...] = dot(mixed_all, ow[layer])
        for j in range(n_tp):
            send_o[layer, j] = acc[rows * j : rows * (j + 1), :].astype(BF)
        waits = exchange(
            "tp", n_tp, me_tp, lambda peer: send_o.at[layer, peer], recv_o.at[layer],
            ox_s.at[layer], ox_r.at[layer],
        )
        total = send_o[layer, me_tp].astype(F32)
        for k, w in enumerate(waits):
            w.wait_recv()
            total = total + recv_o[layer, lax.rem(me_tp + n_tp - 1 - k, n_tp)].astype(F32)
        fresh = (mine[...].astype(F32) + total).astype(BF)
        if layer + 1 < LAYERS:
            tok[...] = fresh
        else:
            out_ref[...] = fresh
    for copy in pending:
        copy.wait_send()


def expand_rows(small, start):
    return small[:, start:].astype(BF)


def state_kernel(
    seqs, zt_ref, wr_ref, st_ref, fresh_ref, nvh_ref, nch_ref, out_ref, tok_ref, nv_ref, nc_ref
):
    zt = zt_ref[0]
    big = NEW * SUB
    write = wr_ref[0, 0].astype(F32)
    row = grid_of((big, STATE), 0)
    rest = grid_of((128 - big, STATE), 0)
    for s in range(seqs):
        picked = jnp.where((row & (SUB - 1)) == s, write, 0.0)
        fading = jnp.where((rest == s) | (rest == SUB + s), 1.0, 0.0)
        right = jnp.concatenate(
            [
                jnp.concatenate([picked, jnp.zeros((128 - big, STATE), F32)], axis=0),
                jnp.concatenate([jnp.zeros((big, STATE), F32), fading], axis=0),
            ],
            axis=1,
        ).astype(BF)
        both = dot(zt, right)
        out_ref[0, s] = both[:, STATE:] * st_ref[0, s] + both[:, :STATE]

    @pl.when((pl.program_id(0) == 0) & (pl.program_id(1) == 0))
    def _():
        tok_ref[...] = fresh_ref[...]
        half = nc_ref.shape[4]
        for s in range(seqs):
            for j in range(CONV - 1):
                at = SUB * j + s
                nv_ref[s, j] = jnp.concatenate(
                    [nvh_ref[l, at : at + 1, :] for l in range(LAYERS)], axis=0
                ).astype(BF)
                for l in range(LAYERS):
                    nc_ref[l, s, j] = jnp.concatenate(
                        [nch_ref[l, at : at + 1, :half], nch_ref[l, at : at + 1, half:]], axis=0
                    ).astype(BF)


def fast_body(
    n_tp, n_dp,
    tokens, lengths, norm_gain, gate_weight, value_weight, vector_weight, step_weight, step_bias,
    decay_rate, value_taps, vector_taps, out_weight, recurrent_state, value_history, vector_history,
):
    rows, feats = tokens.shape
    seqs = lengths.shape[0]
    block = seqs * NEW
    chans = value_weight.shape[2]
    vwide = 2 * vector_weight.shape[3]
    heads_all = step_weight.shape[2]
    state = recurrent_state.reshape(LAYERS, seqs, chans, STATE)
    groups = GROUPS // n_tp
    big = NEW * SUB
    csum = vwide + heads_all + 128
    vm, hb = pl.BlockSpec(memory_space=pltpu.VMEM), pl.BlockSpec(memory_space=pl.ANY)
    dma = pltpu.SemaphoreType.DMA
    each = vwide // 2 // n_tp
    fresh, nvh, nch, zt, wr = pl.pallas_call(
        functools.partial(step_kernel, n_tp, n_dp, (rows, seqs)),
        out_shape=(
            jax.ShapeDtypeStruct((rows, feats), BF),
            jax.ShapeDtypeStruct((LAYERS, (CONV - 1) * SUB, chans), F32),
            jax.ShapeDtypeStruct((LAYERS, (CONV - 1) * SUB, vwide), F32),
            jax.ShapeDtypeStruct((LAYERS, chans, 128), BF),
            jax.ShapeDtypeStruct((LAYERS, groups, big, STATE), BF),
        ),
        in_specs=[vm, pl.BlockSpec(memory_space=pltpu.SMEM)] + [vm] * 7 + [hb] * 6,
        out_specs=(vm,) * 5,
        scratch_shapes=[
            pltpu.VMEM((LAYERS, feats, chans), BF),
            pltpu.VMEM((LAYERS, feats, chans), BF),
            pltpu.VMEM((LAYERS, feats, vwide), BF),
            pltpu.VMEM((LAYERS, feats, 2, vwide // 2), BF),
            pltpu.VMEM((LAYERS, (CONV - 1) * SUB, chans), F32),
            pltpu.VMEM((LAYERS, (CONV - 1) * SUB, vwide), F32),
            pltpu.VMEM((LAYERS, feats, heads_all), BF),
            pltpu.VMEM((LAYERS, chans, feats), BF),
            pltpu.VMEM((LAYERS, seqs, chans, STATE), F32),
            pltpu.VMEM((LAYERS, n_tp, rows, feats), BF),
            pltpu.VMEM((n_tp * rows, feats), F32),
            pltpu.VMEM((rows, feats), BF),
            pltpu.VMEM((LAYERS, n_dp, block, csum), BF),
            pltpu.VMEM((LAYERS, n_dp, block, csum), BF),
            pltpu.VMEM((LAYERS, n_dp, block, chans), BF),
            pltpu.VMEM((LAYERS, n_dp, block, chans), BF),
            pltpu.VMEM((LAYERS, n_dp, block, chans), BF),
            pltpu.VMEM((LAYERS, n_dp, block, chans), BF),
            pltpu.VMEM((LAYERS, n_tp, each, 128), BF),
            pltpu.VMEM((LAYERS, n_tp, each, 128), BF),
            pltpu.VMEM((LAYERS, block, chans), BF),
            pltpu.VMEM((LAYERS, n_dp, block, chans), BF),
            pltpu.VMEM((n_tp * rows, feats), F32),
            pltpu.VMEM((LAYERS, n_tp, rows, feats), BF),
            pltpu.VMEM((LAYERS, n_tp, rows, feats), BF),
            dma((LAYERS, 6)),
            dma((LAYERS,)),
            dma((LAYERS, n_tp)), dma((LAYERS, n_tp)),
            dma((LAYERS, 3, n_dp)), dma((LAYERS, 3, n_dp)),
            dma((LAYERS, n_tp)), dma((LAYERS, n_tp)),
            dma((LAYERS, n_dp)), dma((LAYERS, n_dp)),
            dma((LAYERS, n_tp)), dma((LAYERS, n_tp)),
        ],
        compiler_params=pltpu.CompilerParams(
            collective_id=0, has_side_effects=True, vmem_limit_bytes=56 * 1024 * 1024
        ),
        name="step_kernel",
    )(
        tokens, lengths, norm_gain, step_bias, decay_rate, value_taps, vector_taps,
        jnp.transpose(value_history, (1, 2, 0, 3)), vector_history,
        gate_weight, value_weight, vector_weight, step_weight,
        out_weight, state,
    )
    cut = chans // groups // 2

    def whole_block(shape):
        return pl.BlockSpec(shape, lambda l, c: (0,) * len(shape))

    turned = (seqs, CONV - 1, LAYERS, chans)
    next_state, out, nv, nc = pl.pallas_call(
        functools.partial(state_kernel, seqs),
        grid=(LAYERS, chans // cut),
        out_shape=(
            jax.ShapeDtypeStruct(state.shape, F32),
            jax.ShapeDtypeStruct((rows, feats), BF),
            jax.ShapeDtypeStruct(turned, BF),
            jax.ShapeDtypeStruct(vector_history.shape, BF),
        ),
        in_specs=[
            pl.BlockSpec((1, cut, 128), lambda l, c: (l, c, 0)),
            pl.BlockSpec((1, 1, big, STATE), lambda l, c: (l, c // 2, 0, 0)),
            pl.BlockSpec((1, seqs, cut, STATE), lambda l, c: (l, 0, c, 0)),
            whole_block((rows, feats)),
            whole_block(nvh.shape),
            whole_block(nch.shape),
        ],
        out_specs=(
            pl.BlockSpec((1, seqs, cut, STATE), lambda l, c: (l, 0, c, 0)),
            whole_block((rows, feats)),
            whole_block(turned),
            whole_block(vector_history.shape),
        ),
        name="state_kernel",
    )(zt, wr, state, fresh, nvh, nch)
    return (
        out,
        next_state.reshape(recurrent_state.shape),
        jnp.transpose(nv, (2, 0, 1, 3)),
        nc,
    )


def choose(n_tp, n_dp, *args):
    tokens, lengths = args[0], args[1]
    fits = (
        GROUPS % n_tp == 0
        and args[7].shape[1] * n_tp == HEADS
        and args[5].shape[3] % 128 == 0
        and tokens.shape[1] % 128 == 0
        and tokens.shape[0] % 4 == 0
        and lengths.shape[0] <= SUB
        and args[5].shape[3] // GROUPS >= 16
        and tokens.shape[0] * n_tp == lengths.shape[0] * NEW * n_dp
    )
    if fits:
        return fast_body(n_tp, n_dp, *args)
    return body(*args)


def solution(mesh):
    return jax.shard_map(
        functools.partial(choose, mesh.shape['tp'], mesh.shape['dp']),
        mesh=mesh,
        in_specs=(
            P("tp", "dp"),
            P("dp"),
            P(None, "dp"),
            P(None, "dp", "tp"),
            P(None, "dp", "tp"),
            P(None, "dp", None, "tp"),
            P(None, "dp", None),
            P(None, "tp"),
            P(None, "tp"),
            P(None, None, "tp"),
            P(None, None, None, "tp"),
            P(None, "tp", "dp"),
            P(None, "dp", "tp", None, None),
            P(None, "dp", None, "tp"),
            P(None, "dp", None, None, "tp"),
        ),
        out_specs=(
            P("tp", "dp"),
            P(None, "dp", "tp", None, None),
            P(None, "dp", None, "tp"),
            P(None, "dp", None, None, "tp"),
        ),
        check_vma=False,
    )
```

```python
import functools

import jax
import jax.numpy as jnp
from jax import lax
from jax.experimental import pallas as pl
from jax.experimental.pallas import tpu as pltpu
from jax.sharding import PartitionSpec as P

D = 4096
HEADS = 128
HEAD_DIM = 64
STATE = 128
GROUPS = 16
CONV = 4
NEW = 4
LAYERS = 2


norm_floor = 0.1
highest = lax.Precision.HIGHEST


def short_conv(history, fresh_rows, conv_taps):
    padded = jnp.concatenate([history, fresh_rows], axis=1)
    block_len = fresh_rows.shape[1]
    summed = jnp.zeros(fresh_rows.shape, jnp.float32)
    for offset in range(conv_taps.shape[0]):
        summed = summed + padded[:, offset : offset + block_len].astype(jnp.float32) * conv_taps[
            offset
        ].astype(jnp.float32)
    return (jax.nn.silu(summed), padded)


def state_block(values, write_vec, read_vec, step_sizes, rate_vec, carried_state):
    block_len = values.shape[1]
    cumulative = jnp.cumsum(step_sizes * rate_vec, axis=1)
    causal = jnp.tril(jnp.ones((block_len, block_len), dtype=bool))[None, :, :, None, None]
    log_gap = cumulative[:, :, None] - cumulative[:, None, :]
    decays = jnp.where(causal, jnp.exp(-jnp.where(causal, log_gap, 0.0)), 0.0)
    scores = jnp.einsum("stgn,sugn->stug", read_vec, write_vec, precision=highest)
    weights = scores[..., None] * decays * step_sizes[:, None]
    within = jnp.einsum("stugr,sugrp->stgrp", weights, values, precision=highest)
    carried = (
        jnp.einsum("stgn,sgrpn->stgrp", read_vec, carried_state, precision=highest)
        * jnp.exp(-cumulative)[..., None]
    )
    ending = jnp.exp(cumulative - cumulative[:, -1:]) * step_sizes
    weighted = values * ending[..., None]
    fresh_state = jnp.einsum("sugrp,sugn->sgrpn", weighted, write_vec, precision=highest)
    next_state = carried_state * jnp.exp(-cumulative[:, -1])[..., None, None] + fresh_state
    return (within + carried, next_state)


def collect(token_rows):
    return lax.all_gather(token_rows, "tp", axis=0, tiled=True)


def body(
    tokens,
    lengths,
    norm_gain,
    gate_weight,
    value_weight,
    vector_weight,
    step_weight,
    step_bias,
    decay_rate,
    value_taps,
    vector_taps,
    out_weight,
    recurrent_state,
    value_history,
    vector_history,
):
    local_seqs = lengths.shape[0]
    local_heads = step_bias.shape[1]
    local_tokens = local_seqs * NEW
    heads_group = HEADS // GROUPS
    group_count = max(1, local_heads // heads_group)
    per_group = local_heads // group_count
    live_mask = (jnp.arange(NEW, dtype=jnp.int32)[None, :] < lengths[:, None]).astype(jnp.float32)
    kept_rows = lengths[:, None] + jnp.arange(CONV - 1, dtype=jnp.int32)[None, :]
    picker = (
        kept_rows[:, :, None] == jnp.arange(CONV - 1 + NEW, dtype=jnp.int32)[None, None, :]
    ).astype(jnp.bfloat16)
    head_start = lax.axis_index("tp") * local_heads
    first_group = head_start // heads_group
    token_rows = tokens
    whole = collect(tokens)
    state_list, value_list, vector_list = ([], [], [])
    for ordinal in range(LAYERS):
        widened = whole.astype(jnp.float32)
        squares = jnp.sum(widened * widened, axis=1)
        normed = (widened * norm_gain[ordinal]).astype(jnp.bfloat16)
        own_step = lax.dynamic_slice_in_dim(step_weight[ordinal], head_start, local_heads, 1)
        gate_part = jnp.dot(normed, gate_weight[ordinal], preferred_element_type=jnp.float32)
        value_part = jnp.dot(normed, value_weight[ordinal], preferred_element_type=jnp.float32)
        vector_part = jnp.einsum(
            "td,dkc->tkc", normed, vector_weight[ordinal], preferred_element_type=jnp.float32
        )
        step_part = jnp.dot(normed, own_step, preferred_element_type=jnp.float32)
        gate_sum, value_sum, vector_sum, step_sum, own_squares = (
            lax.psum_scatter(gate_part, "dp", scatter_dimension=0, tiled=True),
            lax.psum_scatter(value_part, "dp", scatter_dimension=0, tiled=True),
            lax.psum_scatter(vector_part, "dp", scatter_dimension=0, tiled=True),
            lax.psum_scatter(step_part, "dp", scatter_dimension=0, tiled=True),
            lax.psum_scatter(squares, "dp", scatter_dimension=0, tiled=True),
        )
        scaling = lax.rsqrt(own_squares / D + norm_floor)[:, None]
        gate = (gate_sum * scaling).astype(jnp.bfloat16)
        value_in = (value_sum * scaling).astype(jnp.bfloat16)
        vector_in = (vector_sum * scaling[:, :, None]).astype(jnp.bfloat16)
        step_in = (step_sum * scaling).astype(jnp.bfloat16)
        step_sizes = (
            jax.nn.softplus(
                step_in.astype(jnp.float32).reshape(local_seqs, NEW, local_heads)
                + step_bias[ordinal]
            )
            * live_mask[:, :, None]
        )
        value_conv, padded_value = short_conv(
            value_history[ordinal], value_in.reshape(local_seqs, NEW, -1), value_taps[ordinal]
        )
        vector_conv, padded_vector = short_conv(
            vector_history[ordinal], vector_in.reshape(local_seqs, NEW, 2, -1), vector_taps[ordinal]
        )
        vector_whole = lax.all_gather(vector_conv, "tp", axis=3, tiled=True)
        arranged = vector_whole.reshape(local_seqs, NEW, 2, STATE, GROUPS)
        own_vectors = lax.dynamic_slice_in_dim(arranged, first_group, group_count, 4)
        write_vec = jnp.swapaxes(own_vectors[:, :, 0], 2, 3)
        read_vec = jnp.swapaxes(own_vectors[:, :, 1], 2, 3)
        output, next_state = state_block(
            value_conv.reshape(local_seqs, NEW, group_count, per_group, HEAD_DIM),
            write_vec,
            read_vec,
            step_sizes.reshape(local_seqs, NEW, group_count, per_group),
            decay_rate[ordinal].reshape(group_count, per_group),
            recurrent_state[ordinal].reshape(local_seqs, group_count, per_group, HEAD_DIM, STATE),
        )
        state_list.append(next_state.reshape(recurrent_state.shape[1:]))
        value_list.append(
            jnp.einsum(
                "sjk,skc->sjc", picker, padded_value, preferred_element_type=jnp.float32
            ).astype(jnp.bfloat16)
        )
        vector_list.append(
            jnp.einsum(
                "sjk,skmc->sjmc", picker, padded_vector, preferred_element_type=jnp.float32
            ).astype(jnp.bfloat16)
        )
        gated = (
            output.reshape(local_seqs, NEW, -1)
            * jax.nn.silu(gate.astype(jnp.float32).reshape(local_seqs, NEW, -1))
            * live_mask[:, :, None]
        )
        mixed = gated.reshape(local_tokens, -1).astype(jnp.bfloat16)
        mixed_all = lax.all_gather(mixed, "dp", axis=0, tiled=True)
        layer_out = out_weight[ordinal]
        update = lax.psum_scatter(
            jnp.dot(mixed_all, layer_out, preferred_element_type=jnp.float32),
            "tp",
            scatter_dimension=0,
            tiled=True,
        )
        token_rows = (token_rows.astype(jnp.float32) + update).astype(jnp.bfloat16)
        if ordinal + 1 < LAYERS:
            whole = collect(token_rows)
    return (token_rows, jnp.stack(state_list), jnp.stack(value_list), jnp.stack(vector_list))


BF = jnp.bfloat16
F32 = jnp.float32
SUB = 8


def one_hot(cond):
    return jnp.where(cond, 1.0, 0.0).astype(BF)


def grid_of(shape, dim):
    return lax.broadcasted_iota(jnp.int32, shape, dim)


def dot(a, b):
    return jnp.dot(a, b, preferred_element_type=F32)


def dot_nt(a, b):
    return lax.dot_general(a, b, (((1,), (1,)), ((), ())), preferred_element_type=F32)


def silu(x):
    return x * (1.0 / (1.0 + jnp.exp(-x)))


def softplus(x):
    return jnp.maximum(x, 0.0) + jnp.log1p(jnp.exp(-jnp.abs(x)))


def conv_rows(old, fresh, taps):
    padded = [old[SUB * k : SUB * (k + 1)] for k in range(CONV - 1)]
    padded = padded + [fresh[SUB * t : SUB * (t + 1)] for t in range(NEW)]
    outs = []
    for t in range(NEW):
        total = padded[t] * taps[0]
        for k in range(1, CONV):
            total = total + padded[t + k] * taps[k]
        outs.append(silu(total))
    return outs, padded


def keep_rows(padded, lens):
    rows = []
    for j in range(CONV - 1):
        row = padded[j]
        for length in range(1, NEW + 1):
            row = jnp.where(lens == length, padded[length + j], row)
        rows.append(row)
    return jnp.concatenate(rows, axis=0)


def step_kernel(
    n_tp, n_dp, sizes,
    tok_ref, lens_ref, gain_ref, bias_ref, rate_ref, vtap_ref, ctap_ref, vhist_ref, chist_ref,
    gw_hbm, vw_hbm, cw_hbm, sw_hbm, ow_hbm, st_hbm,
    out_ref, nvh_ref, nch_ref, zt_ref, wr_ref,
    gw, vw, cw, raw, vhs, chs, sw, ow, st, stb, whole, x32, tok, send_c, recv_c, send_v, recv_v, send_g, recv_g,
    send_w, recv_w, send_m, recv_m, acc, send_o, recv_o,
    load_sem, own_sem, ag_s, ag_r, rs_s, rs_r, vx_s, vx_r, mx_s, mx_r, ox_s, ox_r,
):
    rows, seqs = sizes
    block = seqs * NEW
    chans = vw.shape[2]
    vcols = cw.shape[2] // 2
    me_tp, me_dp = lax.axis_index("tp"), lax.axis_index("dp")
    barrier = pltpu.get_barrier_semaphore()
    for k in range(1, n_tp):
        pl.semaphore_signal(
            barrier, inc=1, device_id={"tp": lax.rem(me_tp + k, n_tp)},
            device_id_type=pl.DeviceIdType.MESH,
        )
    for k in range(1, n_dp):
        pl.semaphore_signal(
            barrier, inc=1, device_id={"dp": lax.rem(me_dp + k, n_dp)},
            device_id_type=pl.DeviceIdType.MESH,
        )
    loads = {}
    for layer in range(LAYERS):
        for slot, (name, src, dst) in enumerate(
            (("c", cw_hbm, raw), ("s", sw_hbm, sw), ("v", vw_hbm, vw), ("g", gw_hbm, gw),
             ("st", st_hbm, st), ("o", ow_hbm, ow))
        ):
            copy = pltpu.make_async_copy(src.at[layer], dst.at[layer], load_sem.at[layer, slot])
            copy.start()
            loads[layer, name] = copy
    pl.semaphore_wait(barrier, n_tp + n_dp - 2)
    pending = []

    def exchange(axis, n, me, source, target, s_sem, r_sem):
        waits = []
        for k in range(1, n):
            peer = lax.rem(me + k, n)
            copy = pltpu.make_async_remote_copy(
                src_ref=source(peer), dst_ref=target.at[me], send_sem=s_sem.at[k],
                recv_sem=r_sem.at[k], device_id={axis: peer},
                device_id_type=pl.DeviceIdType.MESH,
            )
            copy.start()
            pending.append(copy)
            origin = lax.rem(me + n - k, n)
            waits.append(
                pltpu.make_async_remote_copy(
                    src_ref=target.at[origin], dst_ref=target.at[origin], send_sem=s_sem.at[k],
                    recv_sem=r_sem.at[k], device_id={axis: peer},
                    device_id_type=pl.DeviceIdType.MESH,
                )
            )
        return waits

    who = grid_of((SUB, 128), 0)
    lens = jnp.zeros((SUB, 128), jnp.int32)
    for s in range(seqs):
        lens = jnp.where(who == s, lens_ref[s], lens)
    lens = lens[:, 0:1]
    live = [jnp.where(lens > t, 1.0, 0.0) for t in range(NEW)]
    big = NEW * SUB
    pr, pc = grid_of((big, block), 0), grid_of((big, block), 1)
    spread = one_hot(((pr & (SUB - 1)) < seqs) & (pc == (pr & (SUB - 1)) * NEW + (pr >> 3)))
    qr, qc = grid_of((block, big), 0), grid_of((block, big), 1)
    gather = one_hot((qr >> 2) + (qr & (NEW - 1)) * SUB == qc)
    heads_all = sw.shape[2]
    er, ec = grid_of((heads_all, chans), 0), grid_of((heads_all, chans), 1)
    expand = one_hot(er == me_tp * (chans // HEAD_DIM) + ec // HEAD_DIM)
    orow, ocol = grid_of((vcols, vcols), 0), grid_of((vcols, vcols), 1)
    part_n = vcols // GROUPS
    perm = one_hot(ocol == (orow & (part_n - 1)) * GROUPS + orow // part_n)
    local = chans // HEAD_DIM
    widen = one_hot(grid_of((local, chans), 0) == grid_of((local, chans), 1) // HEAD_DIM)
    left = jnp.concatenate([bias_ref[...], rate_ref[...]], axis=0)
    per_head = jnp.zeros((2 * LAYERS, chans), F32)
    for _ in range(3):
        piece = left.astype(BF)
        per_head = per_head + dot(piece, widen)
        left = left - piece.astype(F32)
    groups = GROUPS // n_tp
    per = chans // groups
    seq_of_row = grid_of((big, STATE), 0) & (SUB - 1)

    for layer in range(LAYERS):
        mine = tok_ref if layer == 0 else tok
        wide = whole.at[layer]
        waits = exchange("tp", n_tp, me_tp, lambda peer: mine, wide, ag_s.at[layer], ag_r.at[layer])
        own = pltpu.make_async_copy(mine, wide.at[me_tp], own_sem.at[layer])
        own.start()
        own.wait()
        if layer == 0:
            vhs[...] = jnp.zeros_like(vhs)
            chs[...] = jnp.zeros_like(chs)
            for s in range(seqs):
                for j in range(CONV - 1):
                    row = SUB * j + s
                    pair = vhist_ref[s, j].astype(F32)
                    for l in range(LAYERS):
                        vhs[l, row : row + 1, :] = pair[l : l + 1]
                        both = chist_ref[l, s, j].astype(F32)
                        chs[l, row : row + 1, :] = jnp.concatenate([both[0:1], both[1:2]], axis=1)
        loads[layer, "c"].wait()
        cut = 64

        def untangle(i, carry):
            at = pl.multiple_of(i * cut, cut)
            some = raw[layer, pl.ds(at, cut)].astype(F32)
            cw[layer, pl.ds(at, cut), :] = jnp.concatenate(
                [some[:, 0, :], some[:, 1, :]], axis=1
            ).astype(BF)
            return carry

        lax.fori_loop(0, raw.shape[1] // cut, untangle, 0)
        loads[layer, "st"].wait()
        for s in range(seqs):
            stb[layer, s] = st[layer, s].astype(BF)
        for w in waits:
            w.wait_recv()
        for i in range(n_tp):
            x32[rows * i : rows * (i + 1), :] = wide[i].astype(F32)
        x = x32[...]
        squares = jnp.sum(x * x, axis=1, keepdims=True)
        normed = (x * gain_ref[layer : layer + 1]).astype(BF)

        def scatter(parts, send, recv, which):
            at = 0
            for part in parts:
                width = part.shape[1]
                for d in range(n_dp):
                    send[layer, d, :, at : at + width] = part[block * d : block * (d + 1)].astype(BF)
                at = at + width
            return exchange(
                "dp", n_dp, me_dp, lambda peer: send.at[layer, peer], recv.at[layer],
                rs_s.at[layer, which], rs_r.at[layer, which],
            )

        def settle(waits, send, recv):
            total = send[layer, me_dp].astype(F32)
            for k, w in enumerate(waits):
                w.wait_recv()
                total = total + recv[layer, lax.rem(me_dp + n_dp - 1 - k, n_dp)].astype(F32)
            return total

        vec_part = dot(normed, cw[layer])
        loads[layer, "s"].wait()
        step_part = dot(normed, sw[layer])
        lane = grid_of((rows * n_tp, 128), 1)
        high = squares.astype(BF).astype(F32)
        sq_part = jnp.where(lane == 0, high, jnp.where(lane == 1, squares - high, 0.0))
        waits_c = scatter((vec_part, step_part, sq_part), send_c, recv_c, 0)
        loads[layer, "v"].wait()
        waits_v = scatter((dot(normed, vw[layer]),), send_v, recv_v, 1)
        loads[layer, "g"].wait()
        waits_g = scatter((dot(normed, gw[layer]),), send_g, recv_g, 2)

        sums = settle(waits_c, send_c, recv_c)
        vwide = 2 * vcols
        total_sq = jnp.sum(sums[:, vwide + heads_all :], axis=1, keepdims=True)
        scaling = lax.rsqrt(total_sq / D + norm_floor)
        small = dot(spread, (sums[:, : vwide + heads_all] * scaling).astype(BF))
        conv, padded_vec = conv_rows(
            chs[layer], small[:, :vwide],
            [
                jnp.concatenate([ctap_ref[layer, k, 0:1], ctap_ref[layer, k, 1:2]], axis=1).astype(F32)
                for k in range(CONV)
            ],
        )
        conv = jnp.concatenate(conv, axis=0)
        stacked = jnp.concatenate(
            [conv[:, :vcols], conv[:, vcols:], jnp.zeros((128 - 2 * big, vcols), F32)], axis=0
        ).astype(BF)
        turned = dot_nt(perm, stacked).astype(BF)
        each = vcols // n_tp
        for j in range(n_tp):
            send_w[layer, j] = turned[each * j : each * (j + 1)]
        waits_w = exchange(
            "tp", n_tp, me_tp, lambda peer: send_w.at[layer, peer], recv_w.at[layer],
            vx_s.at[layer], vx_r.at[layer],
        )
        recv_w[layer, me_tp] = send_w[layer, me_tp]

        steps_wide = dot(expand_rows(small, vwide), expand) + per_head[layer : layer + 1]
        steps_wide = softplus(steps_wide)
        step = [steps_wide[SUB * t : SUB * (t + 1)] * live[t] for t in range(NEW)]
        rate = per_head[LAYERS + layer : LAYERS + layer + 1]
        cum = [step[0] * rate]
        for t in range(1, NEW):
            cum.append(cum[-1] + step[t] * rate)
        values_in = dot(spread, (settle(waits_v, send_v, recv_v) * scaling).astype(BF))
        value, padded_val = conv_rows(
            vhs[layer], values_in, [vtap_ref[layer, k : k + 1].astype(F32) for k in range(CONV)]
        )
        stepped = [step[t] * value[t] for t in range(NEW)]
        reach = [
            [jnp.exp(cum[u] - cum[t]) * stepped[u] for u in range(t + 1)] for t in range(NEW)
        ]
        fades = [jnp.exp(-cum[t]) for t in range(NEW)]
        gate_in = dot(spread, (settle(waits_g, send_g, recv_g) * scaling).astype(BF))
        gates = silu(gate_in)
        for w in waits_w:
            w.wait_recv()
        half = each // groups
        y_parts = [[] for _ in range(NEW)]
        for g in range(groups):
            tall = jnp.concatenate(
                [recv_w[layer, i, half * g : half * (g + 1), :].astype(F32) for i in range(n_tp)],
                axis=0,
            )
            flat = tall.T
            write, read = flat[:big], flat[big : 2 * big]
            wr_ref[layer, g] = write.astype(BF)
            carried = jnp.zeros((big, per), F32)
            for s in range(seqs):
                picked = jnp.where(seq_of_row == s, read, 0.0).astype(BF)
                carried = carried + dot_nt(
                    picked, stb[layer, s, per * g : per * (g + 1), :]
                )
            span = slice(per * g, per * (g + 1))
            for t in range(NEW):
                y = carried[SUB * t : SUB * (t + 1)] * fades[t][:, span]
                for u in range(t + 1):
                    score = jnp.sum(
                        read[SUB * t : SUB * (t + 1)] * write[SUB * u : SUB * (u + 1)],
                        axis=1, keepdims=True,
                    )
                    y = y + score * reach[t][u][:, span]
                y_parts[t].append(y)
        mixed = jnp.concatenate(
            [
                jnp.concatenate(y_parts[t], axis=1) * gates[SUB * t : SUB * (t + 1)] * live[t]
                for t in range(NEW)
            ],
            axis=0,
        ).astype(BF)
        send_m[layer] = dot(gather, mixed).astype(BF)
        waits = exchange(
            "dp", n_dp, me_dp, lambda peer: send_m.at[layer], recv_m.at[layer],
            mx_s.at[layer], mx_r.at[layer],
        )
        recv_m[layer, me_dp] = send_m[layer]
        fade = fades[NEW - 1]
        fade_high = fade.astype(BF).astype(F32)
        zrows = jnp.concatenate(
            reach[NEW - 1] + [fade_high, fade - fade_high, jnp.zeros((128 - big - 2 * SUB, chans), F32)],
            axis=0,
        )
        zt_ref[layer] = zrows.T.astype(BF)
        nch_ref[layer] = keep_rows(padded_vec, lens)
        nvh_ref[layer] = keep_rows(padded_val, lens)
        for w in waits:
            w.wait_recv()
        loads[layer, "o"].wait()
        mixed_all = jnp.concatenate([recv_m[layer, d] for d in range(n_dp)], axis=0)
        acc[...] = dot(mixed_all, ow[layer])
        for j in range(n_tp):
            send_o[layer, j] = acc[rows * j : rows * (j + 1), :].astype(BF)
        waits = exchange(
            "tp", n_tp, me_tp, lambda peer: send_o.at[layer, peer], recv_o.at[layer],
            ox_s.at[layer], ox_r.at[layer],
        )
        total = send_o[layer, me_tp].astype(F32)
        for k, w in enumerate(waits):
            w.wait_recv()
            total = total + recv_o[layer, lax.rem(me_tp + n_tp - 1 - k, n_tp)].astype(F32)
        fresh = (mine[...].astype(F32) + total).astype(BF)
        if layer + 1 < LAYERS:
            tok[...] = fresh
        else:
            out_ref[...] = fresh
    for copy in pending:
        copy.wait_send()


def expand_rows(small, start):
    return small[:, start:].astype(BF)


def state_kernel(
    seqs, zt_ref, wr_ref, fresh_ref, nvh_ref, nch_ref, st_hbm, tok_ref, nv_ref, nc_ref, out_hbm,
    old, new, in_sem, out_sem,
):
    reads, writes = [], []
    for l in range(LAYERS):
        for s in range(seqs):
            copy = pltpu.make_async_copy(st_hbm.at[l, s], old.at[l, s], in_sem.at[l, s])
            copy.start()
            reads.append(copy)
    big = NEW * SUB
    row = grid_of((big, STATE), 0)
    rest = grid_of((128 - big, STATE), 0)
    groups = wr_ref.shape[1]
    per = zt_ref.shape[1] // groups
    tok_ref[...] = fresh_ref[...]
    half = nc_ref.shape[4]
    for s in range(seqs):
        for j in range(CONV - 1):
            at = SUB * j + s
            nv_ref[s, j] = jnp.concatenate(
                [nvh_ref[l, at : at + 1, :] for l in range(LAYERS)], axis=0
            ).astype(BF)
            for l in range(LAYERS):
                nc_ref[l, s, j] = jnp.concatenate(
                    [nch_ref[l, at : at + 1, :half], nch_ref[l, at : at + 1, half:]], axis=0
                ).astype(BF)
    for l in range(LAYERS):
        for s in range(seqs):
            reads[l * seqs + s].wait()
            fading = jnp.where((rest == s) | (rest == SUB + s), 1.0, 0.0)
            for g in range(groups):
                write = wr_ref[l, g].astype(F32)
                picked = jnp.where((row & (SUB - 1)) == s, write, 0.0)
                right = jnp.concatenate(
                    [
                        jnp.concatenate([picked, jnp.zeros((128 - big, STATE), F32)], axis=0),
                        jnp.concatenate([jnp.zeros((big, STATE), F32), fading], axis=0),
                    ],
                    axis=1,
                ).astype(BF)
                span = slice(per * g, per * (g + 1))
                both = dot(zt_ref[l, span, :], right)
                new[l, s, span, :] = both[:, STATE:] * old[l, s, span, :] + both[:, :STATE]
            copy = pltpu.make_async_copy(new.at[l, s], out_hbm.at[l, s], out_sem.at[l, s])
            copy.start()
            writes.append(copy)
    for copy in writes:
        copy.wait()


def fast_body(
    n_tp, n_dp,
    tokens, lengths, norm_gain, gate_weight, value_weight, vector_weight, step_weight, step_bias,
    decay_rate, value_taps, vector_taps, out_weight, recurrent_state, value_history, vector_history,
):
    rows, feats = tokens.shape
    seqs = lengths.shape[0]
    block = seqs * NEW
    chans = value_weight.shape[2]
    vwide = 2 * vector_weight.shape[3]
    heads_all = step_weight.shape[2]
    state = recurrent_state.reshape(LAYERS, seqs, chans, STATE)
    groups = GROUPS // n_tp
    big = NEW * SUB
    csum = vwide + heads_all + 128
    vm, hb = pl.BlockSpec(memory_space=pltpu.VMEM), pl.BlockSpec(memory_space=pl.ANY)
    dma = pltpu.SemaphoreType.DMA
    each = vwide // 2 // n_tp
    fresh, nvh, nch, zt, wr = pl.pallas_call(
        functools.partial(step_kernel, n_tp, n_dp, (rows, seqs)),
        out_shape=(
            jax.ShapeDtypeStruct((rows, feats), BF),
            jax.ShapeDtypeStruct((LAYERS, (CONV - 1) * SUB, chans), F32),
            jax.ShapeDtypeStruct((LAYERS, (CONV - 1) * SUB, vwide), F32),
            jax.ShapeDtypeStruct((LAYERS, chans, 128), BF),
            jax.ShapeDtypeStruct((LAYERS, groups, big, STATE), BF),
        ),
        in_specs=[vm, pl.BlockSpec(memory_space=pltpu.SMEM)] + [vm] * 7 + [hb] * 6,
        out_specs=(vm,) * 5,
        scratch_shapes=[
            pltpu.VMEM((LAYERS, feats, chans), BF),
            pltpu.VMEM((LAYERS, feats, chans), BF),
            pltpu.VMEM((LAYERS, feats, vwide), BF),
            pltpu.VMEM((LAYERS, feats, 2, vwide // 2), BF),
            pltpu.VMEM((LAYERS, (CONV - 1) * SUB, chans), F32),
            pltpu.VMEM((LAYERS, (CONV - 1) * SUB, vwide), F32),
            pltpu.VMEM((LAYERS, feats, heads_all), BF),
            pltpu.VMEM((LAYERS, chans, feats), BF),
            pltpu.VMEM((LAYERS, seqs, chans, STATE), F32),
            pltpu.VMEM((LAYERS, seqs, chans, STATE), BF),
            pltpu.VMEM((LAYERS, n_tp, rows, feats), BF),
            pltpu.VMEM((n_tp * rows, feats), F32),
            pltpu.VMEM((rows, feats), BF),
            pltpu.VMEM((LAYERS, n_dp, block, csum), BF),
            pltpu.VMEM((LAYERS, n_dp, block, csum), BF),
            pltpu.VMEM((LAYERS, n_dp, block, chans), BF),
            pltpu.VMEM((LAYERS, n_dp, block, chans), BF),
            pltpu.VMEM((LAYERS, n_dp, block, chans), BF),
            pltpu.VMEM((LAYERS, n_dp, block, chans), BF),
            pltpu.VMEM((LAYERS, n_tp, each, 128), BF),
            pltpu.VMEM((LAYERS, n_tp, each, 128), BF),
            pltpu.VMEM((LAYERS, block, chans), BF),
            pltpu.VMEM((LAYERS, n_dp, block, chans), BF),
            pltpu.VMEM((n_tp * rows, feats), F32),
            pltpu.VMEM((LAYERS, n_tp, rows, feats), BF),
            pltpu.VMEM((LAYERS, n_tp, rows, feats), BF),
            dma((LAYERS, 6)),
            dma((LAYERS,)),
            dma((LAYERS, n_tp)), dma((LAYERS, n_tp)),
            dma((LAYERS, 3, n_dp)), dma((LAYERS, 3, n_dp)),
            dma((LAYERS, n_tp)), dma((LAYERS, n_tp)),
            dma((LAYERS, n_dp)), dma((LAYERS, n_dp)),
            dma((LAYERS, n_tp)), dma((LAYERS, n_tp)),
        ],
        compiler_params=pltpu.CompilerParams(
            collective_id=0, has_side_effects=True, vmem_limit_bytes=56 * 1024 * 1024
        ),
        name="step_kernel",
    )(
        tokens, lengths, norm_gain, step_bias, decay_rate, value_taps, vector_taps,
        jnp.transpose(value_history, (1, 2, 0, 3)), vector_history,
        gate_weight, value_weight, vector_weight, step_weight,
        out_weight, state,
    )
    turned = (seqs, CONV - 1, LAYERS, chans)
    out, nv, nc, next_state = pl.pallas_call(
        functools.partial(state_kernel, seqs),
        out_shape=(
            jax.ShapeDtypeStruct((rows, feats), BF),
            jax.ShapeDtypeStruct(turned, BF),
            jax.ShapeDtypeStruct(vector_history.shape, BF),
            jax.ShapeDtypeStruct(state.shape, F32),
        ),
        in_specs=[vm] * 5 + [hb],
        out_specs=(vm, vm, vm, hb),
        scratch_shapes=[
            pltpu.VMEM(state.shape, F32),
            pltpu.VMEM(state.shape, F32),
            dma((LAYERS, seqs)),
            dma((LAYERS, seqs)),
        ],
        name="state_kernel",
    )(zt, wr, fresh, nvh, nch, state)
    return (
        out,
        next_state.reshape(recurrent_state.shape),
        jnp.transpose(nv, (2, 0, 1, 3)),
        nc,
    )


def choose(n_tp, n_dp, *args):
    tokens, lengths = args[0], args[1]
    fits = (
        GROUPS % n_tp == 0
        and args[7].shape[1] * n_tp == HEADS
        and args[5].shape[3] % 128 == 0
        and tokens.shape[1] % 128 == 0
        and tokens.shape[0] % 4 == 0
        and lengths.shape[0] <= SUB
        and args[5].shape[3] // GROUPS >= 16
        and tokens.shape[0] * n_tp == lengths.shape[0] * NEW * n_dp
    )
    if fits:
        return fast_body(n_tp, n_dp, *args)
    return body(*args)


def solution(mesh):
    return jax.shard_map(
        functools.partial(choose, mesh.shape['tp'], mesh.shape['dp']),
        mesh=mesh,
        in_specs=(
            P("tp", "dp"),
            P("dp"),
            P(None, "dp"),
            P(None, "dp", "tp"),
            P(None, "dp", "tp"),
            P(None, "dp", None, "tp"),
            P(None, "dp", None),
            P(None, "tp"),
            P(None, "tp"),
            P(None, None, "tp"),
            P(None, None, None, "tp"),
            P(None, "tp", "dp"),
            P(None, "dp", "tp", None, None),
            P(None, "dp", None, "tp"),
            P(None, "dp", None, None, "tp"),
        ),
        out_specs=(
            P("tp", "dp"),
            P(None, "dp", "tp", None, None),
            P(None, "dp", None, "tp"),
            P(None, "dp", None, None, "tp"),
        ),
        check_vma=False,
    )
```
